32 devices in a mesh: sp: 16 (over z, x, core), tp: 2 (over y).
Axes of the slice: x: 2, y: 2, z: 4, core: 2. Of those that a mesh axis runs over, the one named last changes fastest.
Arguments:
- stream: bfloat16 [4096, 2048], P('sp'), may hold values from -6 to 6
- doc_ids: int32 [4096], P('sp'), may hold values from 0 to 3, never falling along the last dimension, each value on 1 to 2048 neighbouring positions
- norm_gain: float32 [2, 2048], replicated, may hold values from 0.1 to 1.9
- w_query: bfloat16 [2, 2048, 1024], P(None, None, 'tp'), may hold values from -0.125 to 0.125
- w_key: bfloat16 [2, 2048, 1024], P(None, None, 'tp'), may hold values from -0.125 to 0.125
- w_value: bfloat16 [2, 2048, 1024], P(None, None, 'tp'), may hold values from -0.125 to 0.125
- query_gain: float32 [2, 64], replicated, may hold values from 0.4 to 7
- key_gain: float32 [2, 64], replicated, may hold values from 0.4 to 7
- offset_bias: float32 [2, 16, 8, 16], P(None, 'tp'), may hold values from -4 to 4
- w_output: bfloat16 [2, 1024, 2048], replicated, may hold values from -0.1875 to 0.1875
Outputs:
- result: bfloat16 [4096, 2048], P('sp')
The draws below stay inside these ranges and needn't reach their ends.
Inputs may be any that keep to these rules, and one draw needn't show every extreme that they name: `doc_ids`: numbers never fall along the sequence; each document holds 1 to 2048 positions and one holds exactly 2048.
All inputs are finite; a program needn't handle non-finite values.
Results may differ from the reference program's by a relative error of at most 0.034.
The reference program's roundings to bfloat16 on the way (of `normed`, `queries`, `values`, `weights` and `attended`) count: a program that leaves them out, or rounds other values in their place, can miss the bound.
Values may be sent and summed in bfloat16 or wider, within the bound.
A program may use at most 128 MiB of HBM per device.

```python
import math
import jax
import jax.numpy as jnp
import numpy as np
from jax import lax

D = 2048
HEADS = 16
HEAD_DIM = 64
GRID_W = 64
WIN_ROWS = 8
WIN_COLS = 16
LAYERS = 2
TOKENS = 4096
DOCS = 4
DOC_MOST = 2048


def draw_query_gain(key, part):
    fresh = jax.random.fold_in(key, 11)
    return jnp.clip(1.0 + 0.18 * jax.random.normal(fresh, (LAYERS, HEAD_DIM), jnp.float32), 0.45, 1.55)


def draw_key_gain(key, part):
    fresh = jax.random.fold_in(key, 23)
    return jnp.clip(1.0 + 0.18 * jax.random.normal(fresh, (LAYERS, HEAD_DIM), jnp.float32), 0.45, 1.55)


def block_levels(key, dims, split, smallest, high):
    loudness, own = 1.0, jax.random.fold_in(key, 6)
    for position, shards_of in split:
        heights = jnp.exp(jax.random.uniform(jax.random.fold_in(own, position), (shards_of,), jnp.float32, smallest / len(split), high / len(split)))
        loudness = loudness * jnp.repeat(heights, dims[position] // shards_of).reshape([-1 if axis == position else 1 for axis in range(len(dims))])
    return loudness


def length_profile(number_of, total, reach, slope):
    portions = [(1 << 20) // math.isqrt(rank ** slope) + 1 for rank in range(2, number_of + 1)]
    spare, given = total - reach - (number_of - 1), [1] * (number_of - 1)
    while spare > 0:
        candidates = [i for i in range(number_of - 1) if given[i] < reach]
        whole, remaining = sum([portions[i] for i in candidates]), spare
        for i in candidates:
            addition = min(reach - given[i], max(1, remaining * portions[i] // whole), spare)
            given[i] = given[i] + addition
            spare = spare - addition
    return np.array([reach] + given)


def uneven_parts(rng, count, total, bound, lean):
    if count == 2:
        one = jax.random.randint(rng, (), max(1, total - bound), min(bound, total - 1) + 1)
        return jnp.stack([one, total - one])
    tallies = jnp.asarray(length_profile(count, total, bound, lean), jnp.int32)
    twos = (count - 1) // 2
    donor, receiver = tallies[1:1 + 2 * twos:2], tallies[2:2 + 2 * twos:2]
    room = jnp.minimum(donor - 1, bound - receiver)
    passed = jax.random.randint(jax.random.fold_in(rng, 1), (twos,), 0, 1 << 20) % (room + 1)
    tallies = tallies.at[1:1 + 2 * twos:2].set(donor - passed).at[2:2 + 2 * twos:2].set(receiver + passed)
    return tallies[jax.random.permutation(jax.random.fold_in(rng, 2), count)]


def bell_draw(rng, extent, spread, bound, split=(), kind=jnp.bfloat16):
    values = spread * jax.random.normal(rng, extent, jnp.float32)
    if split:
        values = values * block_levels(rng, extent, split, -0.22, 0.18)
    return jnp.clip(values, -bound, bound).astype(kind)


def setup_inputs(seed: int = 0) -> dict:
    key_list = jax.random.split(jax.random.key(seed), 11)
    return {
        "stream": bell_draw(key_list[0], (TOKENS, D), 1.0, 6.0, ((0, 16),)),
        "doc_ids": jnp.searchsorted(jnp.cumsum(uneven_parts(key_list[1], DOCS, TOKENS, DOC_MOST, 0)), jnp.arange(TOKENS), side="right").astype(jnp.int32),
        "norm_gain": jnp.clip(1.0 + 0.18 * jax.random.normal(key_list[2], (LAYERS, D), jnp.float32), 0.1, 1.9),
        "w_query": bell_draw(key_list[3], (LAYERS, D, HEADS * HEAD_DIM), D ** -0.5, 0.125, ((2, 2),)),
        "w_key": bell_draw(key_list[4], (LAYERS, D, HEADS * HEAD_DIM), D ** -0.5, 0.125, ((2, 2),)),
        "w_value": bell_draw(key_list[5], (LAYERS, D, HEADS * HEAD_DIM), D ** -0.5, 0.125, ((2, 2),)),
        "query_gain": draw_query_gain(jax.random.fold_in(key_list[10], 71), 0),
        "key_gain": draw_key_gain(jax.random.fold_in(key_list[10], 71), 0),
        "offset_bias": bell_draw(key_list[8], (LAYERS, HEADS, WIN_ROWS, WIN_COLS), 1.0, 4.0, ((1, 2),), jnp.float32),
        "w_output": bell_draw(key_list[9], (LAYERS, HEADS * HEAD_DIM, D), (HEADS * HEAD_DIM) ** -0.5, 0.1875),
    }


eps = 1e-06

def head_norm(raw_rows, gain_row):
    split_rows = raw_rows.reshape(raw_rows.shape[0], -1, HEAD_DIM)
    inverse = lax.rsqrt(lax.optimization_barrier(jnp.mean(split_rows * split_rows, axis=-1, keepdims=True)) + eps)
    return (split_rows * inverse * gain_row).astype(jnp.bfloat16).reshape(raw_rows.shape)

def offset_table(head_bias):
    key_reach = 2 * WIN_COLS - 1
    offsets = jnp.arange(key_reach, dtype=jnp.int32)[None, :] - jnp.arange(WIN_COLS, dtype=jnp.int32)[:, None]
    inside = (offsets >= 0) & (offsets < WIN_COLS)
    one_hot = (offsets[:, :, None] == jnp.arange(WIN_COLS, dtype=jnp.int32)[None, None, :]).astype(jnp.float32)
    lookup = jnp.einsum('hjc,qkc->qhjk', head_bias, one_hot, precision=lax.Precision.HIGHEST)
    return (lookup, inside)

def window_attend(queries, pair_pad, query_marks, mark_pad, head_bias):
    heads_here = head_bias.shape[0]
    tokens_here = queries.shape[0]
    grid_rows = tokens_here // GRID_W
    col_blocks = GRID_W // WIN_COLS
    key_reach = 2 * WIN_COLS - 1
    margin = WIN_COLS // 2
    col_pad = ((0, 0), (margin, WIN_COLS - 1 - margin))
    pair_grid = jnp.pad(pair_pad.reshape(grid_rows + WIN_ROWS, GRID_W, -1), col_pad + ((0, 0),))
    mark_grid = jnp.pad(mark_pad.reshape(grid_rows + WIN_ROWS, GRID_W), col_pad)
    pair_band = jnp.stack([pair_grid[row_shift:row_shift + grid_rows] for row_shift in range(WIN_ROWS)], axis=1)
    mark_band = jnp.stack([mark_grid[row_shift:row_shift + grid_rows] for row_shift in range(WIN_ROWS)], axis=1)
    pair_win = jnp.stack([pair_band[:, :, col_block * WIN_COLS:col_block * WIN_COLS + key_reach] for col_block in range(col_blocks)], axis=2)
    mark_win = jnp.stack([mark_band[:, :, col_block * WIN_COLS:col_block * WIN_COLS + key_reach] for col_block in range(col_blocks)], axis=2)
    pair_win = pair_win.reshape(grid_rows, WIN_ROWS, col_blocks, key_reach, 2, heads_here, HEAD_DIM)
    key_win = pair_win[:, :, :, :, 0]
    value_win = pair_win[:, :, :, :, 1]
    query_grid = queries.reshape(grid_rows, col_blocks, WIN_COLS, heads_here, HEAD_DIM)
    scores = jnp.einsum('rbqhd,rjbkhd->rbqhjk', query_grid.astype(jnp.float32), key_win.astype(jnp.float32))
    lookup, inside = offset_table(head_bias)
    own_marks = query_marks.reshape(grid_rows, col_blocks, WIN_COLS)
    same_doc = mark_win.transpose(0, 2, 1, 3)[:, :, None, :, :] == own_marks[:, :, :, None, None]
    allowed = same_doc & inside[None, None, :, None, :]
    scores = scores * HEAD_DIM ** (-0.5) + lookup[None, None]
    scores = jnp.where(allowed[:, :, :, None], scores, -jnp.inf)
    highest = lax.optimization_barrier(jnp.max(scores, axis=(4, 5), keepdims=True))
    shifted_exp = jnp.exp(scores - highest)
    weights = (shifted_exp / lax.optimization_barrier(jnp.sum(shifted_exp, axis=(4, 5), keepdims=True))).astype(jnp.bfloat16)
    mixed = jnp.einsum('rbqhjk,rjbkhd->rbqhd', weights.astype(jnp.float32), value_win.astype(jnp.float32))
    return mixed.astype(jnp.bfloat16).reshape(tokens_here, heads_here * HEAD_DIM)

def reference(stream, doc_ids, norm_gain, w_query, w_key, w_value, query_gain, key_gain, offset_bias, w_output):
    hidden = stream
    marks = doc_ids + 1
    halo_tokens = WIN_ROWS // 2 * GRID_W
    mark_pad = jnp.pad(marks, (halo_tokens, halo_tokens))
    for layer_index in range(LAYERS):
        token_rows = hidden.astype(jnp.float32)
        inv_rms = lax.rsqrt(lax.optimization_barrier(jnp.mean(token_rows * token_rows, axis=-1, keepdims=True)) + eps)
        normed = (token_rows * inv_rms * norm_gain[layer_index]).astype(jnp.bfloat16)
        queries = head_norm(jnp.dot(normed, w_query[layer_index], preferred_element_type=jnp.float32), query_gain[layer_index])
        key_rows = head_norm(jnp.dot(normed, w_key[layer_index], preferred_element_type=jnp.float32), key_gain[layer_index])
        value_rows = jnp.dot(normed, w_value[layer_index], preferred_element_type=jnp.float32).astype(jnp.bfloat16)
        layer_bias = offset_bias[layer_index]

        def one_head(head_number):
            start_col = head_number * HEAD_DIM
            head_query = lax.dynamic_slice_in_dim(queries, start_col, HEAD_DIM, 1)
            head_pairs = jnp.concatenate([lax.dynamic_slice_in_dim(key_rows, start_col, HEAD_DIM, 1), lax.dynamic_slice_in_dim(value_rows, start_col, HEAD_DIM, 1)], axis=1)
            pair_pad = jnp.pad(head_pairs, ((halo_tokens, halo_tokens), (0, 0)))
            head_bias = lax.dynamic_slice_in_dim(layer_bias, head_number, 1, 0)
            return window_attend(head_query, pair_pad, marks, mark_pad, head_bias)
        per_head = lax.map(one_head, jnp.arange(HEADS, dtype=jnp.int32))
        attended = per_head.transpose(1, 0, 2).reshape(hidden.shape[0], HEADS * HEAD_DIM)
        projected = jnp.dot(attended, w_output[layer_index], preferred_element_type=jnp.float32)
        hidden = (hidden.astype(jnp.float32) + projected).astype(jnp.bfloat16)
    return hidden
```

```python
import functools

import jax
import jax.numpy as jnp
from jax import lax
from jax.experimental import pallas as pl
from jax.experimental.pallas import tpu as pltpu
from jax.sharding import PartitionSpec as P

HEAD_DIM = 64
GRID_W = 64
WIN_ROWS = 8
WIN_COLS = 16
EPS = 1e-06
LOW = WIN_ROWS // 2 * GRID_W
HIGH = (WIN_ROWS - WIN_ROWS // 2 - 1) * GRID_W
KEYS = WIN_ROWS * GRID_W
NEG = -1e30
MESH = pl.DeviceIdType.MESH
F32 = jnp.float32
BF16 = jnp.bfloat16


def kernel(
    sp_size,
    tp_size,
    stream_ref,
    doc_ref,
    norm_gain_ref,
    wq_hbm,
    wk_hbm,
    wv_hbm,
    q_gain_ref,
    k_gain_ref,
    bias_ref,
    wo_hbm,
    out_ref,
    wbuf,
    wobuf,
    hbuf,
    nbuf,
    qbuf,
    kbuf,
    vbuf,
    att,
    acc,
    table,
    maskbuf,
    marks,
    w_sem,
    wo_sem,
    mark_send,
    mark_recv,
    k_send,
    k_recv,
    v_send,
    v_recv,
    a_send,
    a_recv,
):
    layers, width, head_width = wk_hbm.shape
    tokens = stream_ref.shape[0]
    rows = tokens // GRID_W
    group = min(128, head_width)
    per_group = group // HEAD_DIM
    groups = head_width // group
    me = lax.axis_index("sp")
    mine = lax.axis_index("tp")
    has_prev = me > 0
    has_next = me < sp_size - 1
    prev = lax.rem(me + sp_size - 1, sp_size)
    following = lax.rem(me + 1, sp_size)

    def w_copy(layer, which):
        source = (wq_hbm, wk_hbm, wv_hbm)[which]
        return pltpu.make_async_copy(
            source.at[layer], wbuf.at[layer, which], w_sem.at[layer, which]
        )

    def wo_copy(layer):
        return pltpu.make_async_copy(wo_hbm.at[layer], wobuf.at[layer], wo_sem.at[layer])

    w_copy(0, 1).start()
    w_copy(0, 2).start()

    barrier = pltpu.get_barrier_semaphore()

    @pl.when(has_prev)
    def _():
        pl.semaphore_signal(barrier, inc=1, device_id={"sp": prev}, device_id_type=MESH)

    @pl.when(has_next)
    def _():
        pl.semaphore_signal(barrier, inc=1, device_id={"sp": following}, device_id_type=MESH)

    for step in range(1, tp_size):
        pl.semaphore_signal(
            barrier,
            inc=1,
            device_id={"tp": lax.rem(mine + step, tp_size)},
            device_id_type=MESH,
        )

    def halo(buf, layer, send, recv):
        here = buf.at[layer]
        ahead = pltpu.make_async_remote_copy(
            src_ref=here.at[pl.ds(LOW + tokens - LOW, LOW)],
            dst_ref=here.at[pl.ds(0, LOW)],
            send_sem=send.at[layer, 0],
            recv_sem=recv.at[layer, 0],
            device_id={"sp": following},
            device_id_type=MESH,
        )
        back = pltpu.make_async_remote_copy(
            src_ref=here.at[pl.ds(LOW, HIGH)],
            dst_ref=here.at[pl.ds(LOW + tokens, HIGH)],
            send_sem=send.at[layer, 1],
            recv_sem=recv.at[layer, 1],
            device_id={"sp": prev},
            device_id_type=MESH,
        )
        return ahead, back

    def mark_copies():
        ahead = pltpu.make_async_remote_copy(
            src_ref=doc_ref,
            dst_ref=marks.at[0],
            send_sem=mark_send.at[0],
            recv_sem=mark_recv.at[0],
            device_id={"sp": following},
            device_id_type=MESH,
        )
        back = pltpu.make_async_remote_copy(
            src_ref=doc_ref,
            dst_ref=marks.at[1],
            send_sem=mark_send.at[1],
            recv_sem=mark_recv.at[1],
            device_id={"sp": prev},
            device_id_type=MESH,
        )
        return ahead, back

    def start_both(pair):
        @pl.when(has_next)
        def _():
            pair[0].start()

        @pl.when(has_prev)
        def _():
            pair[1].start()

    def wait_send_both(pair):
        @pl.when(has_next)
        def _():
            pair[0].wait_send()

        @pl.when(has_prev)
        def _():
            pair[1].wait_send()

    def wait_low(pair):
        @pl.when(has_prev)
        def _():
            pair[0].wait_recv()

    def wait_high(pair):
        @pl.when(has_next)
        def _():
            pair[1].wait_recv()

    def att_copy(layer, row, step):
        block = att.at[layer, mine, pl.ds(row * GRID_W, GRID_W)]
        return pltpu.make_async_remote_copy(
            src_ref=block,
            dst_ref=block,
            send_sem=a_send.at[layer, step - 1, row],
            recv_sem=a_recv.at[layer, step - 1, row],
            device_id={"tp": lax.rem(mine + step, tp_size)},
            device_id_type=MESH,
        )

    @pl.when(jnp.logical_not(has_prev))
    def _():
        marks[0] = jnp.full((1, tokens), -1, jnp.int32)
        kbuf[:, 0:LOW, :] = jnp.zeros((layers, LOW, head_width), BF16)
        vbuf[:, 0:LOW, :] = jnp.zeros((layers, LOW, head_width), BF16)

    @pl.when(jnp.logical_not(has_next))
    def _():
        marks[1] = jnp.full((1, tokens), -1, jnp.int32)
        kbuf[:, LOW + tokens :, :] = jnp.zeros((layers, HIGH, head_width), BF16)
        vbuf[:, LOW + tokens :, :] = jnp.zeros((layers, HIGH, head_width), BF16)

    span = min(256, head_width)
    head_row = lax.broadcasted_iota(jnp.int32, (span, span), 0) // HEAD_DIM
    head_col = lax.broadcasted_iota(jnp.int32, (span, span), 1) // HEAD_DIM
    averager = jnp.where(head_row == head_col, 1.0 / HEAD_DIM, 0.0).astype(BF16)

    def head_norm(raw, gain):
        squares = raw * raw
        coarse = squares.astype(BF16)
        fine = (squares - coarse.astype(F32)).astype(BF16)
        mean = jnp.dot(coarse, averager, preferred_element_type=F32) + jnp.dot(
            fine, averager, preferred_element_type=F32
        )
        return (raw * lax.rsqrt(mean + EPS) * gain).astype(BF16)

    def project(layer, which, write):
        for start in range(0, head_width, span):
            write(
                start,
                jnp.dot(
                    nbuf[...],
                    wbuf[layer, which, :, start : start + span],
                    preferred_element_type=F32,
                ),
            )

    def build_tables():
        query_col = lax.broadcasted_iota(jnp.int32, (GRID_W, 128), 0)
        key_col = lax.rem(lax.broadcasted_iota(jnp.int32, (GRID_W, 128), 1), GRID_W)
        offset = key_col - query_col + WIN_COLS // 2
        band = (offset >= 0) & (offset < WIN_COLS)
        heads = head_width // HEAD_DIM
        tiles = KEYS // 128
        for layer in range(layers):
            for head in range(heads):
                for tile in range(tiles):
                    index = (layer * heads + head) * tiles + tile
                    line = jnp.broadcast_to(bias_ref[index : index + 1, :], (GRID_W, 128))
                    line = pltpu.roll(line, 128 - WIN_COLS // 2, 1, stride=1, stride_axis=0)
                    table[
                        layer,
                        head * GRID_W : (head + 1) * GRID_W,
                        tile * 128 : (tile + 1) * 128,
                    ] = jnp.where(band, line, NEG)

    def build_masks():
        own = doc_ref[...]
        every = jnp.concatenate([marks[0], own, marks[1]], axis=1).astype(F32)
        own_rows = jnp.broadcast_to(own.astype(F32), (128, tokens)).T
        base = tokens - LOW
        for row in range(rows):
            left = base + row * GRID_W
            keys_here = every[:, left : left + KEYS]
            queries_here = own_rows[row * GRID_W : (row + 1) * GRID_W, 0:1]
            maskbuf[row] = jnp.where(queries_here == keys_here, 0.0, NEG)

    lane = lax.broadcasted_iota(jnp.int32, (GRID_W, group), 1)

    def attend_row(layer, row):
        low = row * GRID_W
        for g in range(groups):
            cols = slice(g * group, (g + 1) * group)
            q = qbuf[low : low + GRID_W, cols]
            if per_group == 2:
                zero = jnp.zeros_like(q)
                q = jnp.concatenate(
                    [
                        jnp.where(lane < HEAD_DIM, q, zero),
                        jnp.where(lane >= HEAD_DIM, q, zero),
                    ],
                    axis=0,
                )
            k = kbuf[layer, low : low + KEYS, cols]
            v = vbuf[layer, low : low + KEYS, cols]
            scores = lax.dot_general(
                q, k, (((1,), (1,)), ((), ())), preferred_element_type=F32
            )
            exps, sums = [], []
            for i in range(per_group):
                head = g * per_group + i
                s = (
                    scores[i * GRID_W : (i + 1) * GRID_W]
                    + table[layer, head * GRID_W : (head + 1) * GRID_W, :]
                    + maskbuf[row]
                )
                e = jnp.exp(s - jnp.max(s, axis=-1, keepdims=True))
                sums.append(jnp.sum(e, axis=-1, keepdims=True))
                exps.append(e.astype(BF16))
            weights = exps[0] if per_group == 1 else jnp.concatenate(exps, axis=0)
            mixed = jnp.dot(weights, v, preferred_element_type=F32)
            parts = [
                mixed[i * GRID_W : (i + 1) * GRID_W] / sums[i] for i in range(per_group)
            ]
            result = (
                parts[0] if per_group == 1 else jnp.where(lane < HEAD_DIM, parts[0], parts[1])
            )
            att[layer, mine, low : low + GRID_W, cols] = result.astype(BF16)

    chunk = 512
    for layer in range(layers):
        source = stream_ref if layer == 0 else hbuf
        target = out_ref if layer == layers - 1 else hbuf

        block = 32

        def norm_rows(i, carry):
            at = pl.ds(pl.multiple_of(i * block, block), block)
            x = source[at, :].astype(F32)
            inverse = lax.rsqrt(jnp.mean(x * x, axis=-1, keepdims=True) + EPS)
            nbuf[at, :] = (x * inverse * norm_gain_ref[layer : layer + 1, :]).astype(BF16)
            return carry

        lax.fori_loop(0, tokens // block, norm_rows, 0)

        k_gain = k_gain_ref[layer : layer + 1, :]
        q_gain = q_gain_ref[layer : layer + 1, :] * HEAD_DIM ** (-0.5)

        w_copy(layer, 1).wait()
        if layer == 0:
            w_copy(0, 0).start()
            wo_copy(0).start()

        def write_k(start, raw):
            kbuf[layer, LOW : LOW + tokens, start : start + span] = head_norm(
                raw, k_gain[:, start : start + span]
            )

        project(layer, 1, write_k)
        if layer == 0:
            degree = has_prev.astype(jnp.int32) + has_next.astype(jnp.int32) + (tp_size - 1)
            pl.semaphore_wait(barrier, degree)
            start_both(mark_copies())
        start_both(halo(kbuf, layer, k_send, k_recv))

        w_copy(layer, 2).wait()

        def write_v(start, raw):
            vbuf[layer, LOW : LOW + tokens, start : start + span] = raw.astype(BF16)

        project(layer, 2, write_v)
        start_both(halo(vbuf, layer, v_send, v_recv))
        if layer == 0:
            for later in range(1, layers):
                for which in (1, 2, 0):
                    w_copy(later, which).start()
                wo_copy(later).start()

        w_copy(layer, 0).wait()

        def write_q(start, raw):
            qbuf[:, start : start + span] = head_norm(raw, q_gain[:, start : start + span])

        project(layer, 0, write_q)
        if layer == 0:
            build_tables()
            wait_low(mark_copies())
            wait_high(mark_copies())
            build_masks()

        wait_low(halo(kbuf, layer, k_send, k_recv))
        wait_low(halo(vbuf, layer, v_send, v_recv))
        for row in range(rows):
            if row == 1:
                wait_high(halo(kbuf, layer, k_send, k_recv))
                wait_high(halo(vbuf, layer, v_send, v_recv))
            attend_row(layer, row)
            for step in range(1, tp_size):
                att_copy(layer, row, step).start()

        wo_copy(layer).wait()

        def out_part(owner, start):
            return jnp.dot(
                att[layer, owner],
                wobuf[
                    layer,
                    pl.ds(pl.multiple_of(owner * head_width, head_width), head_width),
                    start : start + chunk,
                ],
                preferred_element_type=F32,
            )

        for start in range(0, width, chunk):
            cols = slice(start, start + chunk)
            acc[:, cols] = source[:, cols].astype(F32) + out_part(mine, start)
        for step in range(1, tp_size):
            for row in range(rows):
                att_copy(layer, row, step).wait_recv()
            owner = lax.rem(mine + tp_size - step, tp_size)
            for start in range(0, width, chunk):
                cols = slice(start, start + chunk)
                total = acc[:, cols] + out_part(owner, start)
                if step == tp_size - 1:
                    target[:, cols] = total.astype(BF16)
                else:
                    acc[:, cols] = total
        if tp_size == 1:
            target[...] = acc[...].astype(BF16)

    wait_send_both(mark_copies())
    for layer in range(layers):
        wait_send_both(halo(kbuf, layer, k_send, k_recv))
        wait_send_both(halo(vbuf, layer, v_send, v_recv))
        for step in range(1, tp_size):
            for row in range(rows):
                att_copy(layer, row, step).wait_send()


def on_device(
    sp_size,
    tp_size,
    stream,
    doc_ids,
    norm_gain,
    w_query,
    w_key,
    w_value,
    query_gain,
    key_gain,
    offset_bias,
    w_output,
):
    tokens, width = stream.shape
    layers, _, head_width = w_query.shape
    heads = head_width // HEAD_DIM
    rows = tokens // GRID_W
    all_width = w_output.shape[1]
    bias = jnp.pad(offset_bias, ((0, 0), (0, 0), (0, 0), (0, GRID_W - WIN_COLS)))
    bias = bias.reshape(layers * heads * (KEYS // 128), 128)
    vmem = pl.BlockSpec(memory_space=pltpu.VMEM)
    hbm = pl.BlockSpec(memory_space=pl.ANY)
    sem = pltpu.SemaphoreType.DMA
    peers = max(1, tp_size - 1)
    return pl.pallas_call(
        functools.partial(kernel, sp_size, tp_size),
        out_shape=jax.ShapeDtypeStruct((tokens, width), BF16),
        in_specs=[vmem, vmem, vmem, hbm, hbm, hbm, vmem, vmem, vmem, hbm],
        out_specs=vmem,
        scratch_shapes=[
            pltpu.VMEM((layers, 3, width, head_width), BF16),
            pltpu.VMEM((layers, all_width, width), BF16),
            pltpu.VMEM((tokens, width), BF16),
            pltpu.VMEM((tokens, width), BF16),
            pltpu.VMEM((tokens, head_width), BF16),
            pltpu.VMEM((layers, LOW + tokens + HIGH, head_width), BF16),
            pltpu.VMEM((layers, LOW + tokens + HIGH, head_width), BF16),
            pltpu.VMEM((layers, tp_size, tokens, head_width), BF16),
            pltpu.VMEM((tokens, width), F32),
            pltpu.VMEM((layers, heads * GRID_W, KEYS), F32),
            pltpu.VMEM((rows, GRID_W, KEYS), F32),
            pltpu.VMEM((2, 1, tokens), jnp.int32),
            sem((layers, 3)),
            sem((layers,)),
            sem((2,)),
            sem((2,)),
            sem((layers, 2)),
            sem((layers, 2)),
            sem((layers, 2)),
            sem((layers, 2)),
            sem((layers, peers, rows)),
            sem((layers, peers, rows)),
        ],
        compiler_params=pltpu.CompilerParams(
            collective_id=0, has_side_effects=True, vmem_limit_bytes=60 * 1024 * 1024
        ),
    )(
        stream,
        doc_ids.reshape(1, tokens),
        norm_gain,
        w_query,
        w_key,
        w_value,
        jnp.tile(query_gain, (1, heads)),
        jnp.tile(key_gain, (1, heads)),
        bias,
        w_output,
    )


def solution(mesh):
    return jax.shard_map(
        functools.partial(on_device, mesh.shape["sp"], mesh.shape["tp"]),
        mesh=mesh,
        in_specs=(
            P("sp", None),
            P("sp"),
            P(),
            P(None, None, "tp"),
            P(None, None, "tp"),
            P(None, None, "tp"),
            P(),
            P(),
            P(None, "tp", None, None),
            P(),
        ),
        out_specs=P("sp", None),
        check_vma=False,
    )
```

```python
import functools

import jax
import jax.numpy as jnp
from jax import lax
from jax.experimental import pallas as pl
from jax.experimental.pallas import tpu as pltpu
from jax.sharding import PartitionSpec as P

HEAD_DIM = 64
GRID_W = 64
WIN_ROWS = 8
WIN_COLS = 16
EPS = 1e-06
LOW = WIN_ROWS // 2 * GRID_W
HIGH = (WIN_ROWS - WIN_ROWS // 2 - 1) * GRID_W
KEYS = WIN_ROWS * GRID_W
NEG = -1e30
MESH = pl.DeviceIdType.MESH
F32 = jnp.float32
BF16 = jnp.bfloat16


def kernel(
    sp_size,
    tp_size,
    stream_ref,
    doc_ref,
    norm_gain_ref,
    wq_hbm,
    wk_hbm,
    wv_hbm,
    q_gain_ref,
    k_gain_ref,
    bias_ref,
    wo_hbm,
    out_ref,
    wqbuf,
    wkvbuf,
    wobuf,
    hbuf,
    nbuf,
    qbuf,
    kvbuf,
    att,
    acc,
    table,
    maskbuf,
    marks,
    lines,
    wq_sem,
    wkv_sem,
    wo_sem,
    mark_send,
    mark_recv,
    kv_send,
    kv_recv,
    a_send,
    a_recv,
):
    layers, width, head_width = wk_hbm.shape
    tokens = stream_ref.shape[0]
    rows = tokens // GRID_W
    group = min(128, head_width)
    per_group = group // HEAD_DIM
    groups = head_width // group
    paired = group == 128
    me = lax.axis_index("sp")
    mine = lax.axis_index("tp")
    has_prev = me > 0
    has_next = me < sp_size - 1
    prev = lax.rem(me + sp_size - 1, sp_size)
    following = lax.rem(me + 1, sp_size)

    def wq_copy(layer):
        return pltpu.make_async_copy(wq_hbm.at[layer], wqbuf.at[layer], wq_sem.at[layer])

    def wkv_copy(layer, g, part):
        source = (wk_hbm, wv_hbm)[part].at[layer]
        if paired:
            source = source.at[:, pl.ds(g * group, group)]
            target = wkvbuf.at[layer, g, :, pl.ds(part * group, group)]
        else:
            target = wkvbuf.at[layer, part]
        return pltpu.make_async_copy(source, target, wkv_sem.at[layer, g, part])

    def wo_copy(layer):
        return pltpu.make_async_copy(wo_hbm.at[layer], wobuf.at[layer], wo_sem.at[layer])

    for g in range(groups):
        for part in range(2):
            wkv_copy(0, g, part).start()

    barrier = pltpu.get_barrier_semaphore()

    @pl.when(has_prev)
    def _():
        pl.semaphore_signal(barrier, inc=1, device_id={"sp": prev}, device_id_type=MESH)

    @pl.when(has_next)
    def _():
        pl.semaphore_signal(barrier, inc=1, device_id={"sp": following}, device_id_type=MESH)

    for step in range(1, tp_size):
        pl.semaphore_signal(
            barrier,
            inc=1,
            device_id={"tp": lax.rem(mine + step, tp_size)},
            device_id_type=MESH,
        )

    def halo(layer, g):
        here = kvbuf.at[layer, g]
        ahead = pltpu.make_async_remote_copy(
            src_ref=here.at[pl.ds(tokens, LOW)],
            dst_ref=here.at[pl.ds(0, LOW)],
            send_sem=kv_send.at[layer, g, 0],
            recv_sem=kv_recv.at[layer, g, 0],
            device_id={"sp": following},
            device_id_type=MESH,
        )
        back = pltpu.make_async_remote_copy(
            src_ref=here.at[pl.ds(LOW, HIGH)],
            dst_ref=here.at[pl.ds(LOW + tokens, HIGH)],
            send_sem=kv_send.at[layer, g, 1],
            recv_sem=kv_recv.at[layer, g, 1],
            device_id={"sp": prev},
            device_id_type=MESH,
        )
        return ahead, back

    def mark_copies():
        ahead = pltpu.make_async_remote_copy(
            src_ref=doc_ref,
            dst_ref=marks.at[0],
            send_sem=mark_send.at[0],
            recv_sem=mark_recv.at[0],
            device_id={"sp": following},
            device_id_type=MESH,
        )
        back = pltpu.make_async_remote_copy(
            src_ref=doc_ref,
            dst_ref=marks.at[1],
            send_sem=mark_send.at[1],
            recv_sem=mark_recv.at[1],
            device_id={"sp": prev},
            device_id_type=MESH,
        )
        return ahead, back

    def start_both(pair):
        @pl.when(has_next)
        def _():
            pair[0].start()

        @pl.when(has_prev)
        def _():
            pair[1].start()

    def wait_send_both(pair):
        @pl.when(has_next)
        def _():
            pair[0].wait_send()

        @pl.when(has_prev)
        def _():
            pair[1].wait_send()

    def wait_low(pair):
        @pl.when(has_prev)
        def _():
            pair[0].wait_recv()

    def wait_high(pair):
        @pl.when(has_next)
        def _():
            pair[1].wait_recv()

    def att_copy(layer, g, step):
        block = att.at[layer, mine]
        if paired:
            block = block.at[:, pl.ds(g * group, group)]
        return pltpu.make_async_remote_copy(
            src_ref=block,
            dst_ref=block,
            send_sem=a_send.at[layer, step - 1, g],
            recv_sem=a_recv.at[layer, step - 1, g],
            device_id={"tp": lax.rem(mine + step, tp_size)},
            device_id_type=MESH,
        )

    @pl.when(jnp.logical_not(has_prev))
    def _():
        marks[0] = jnp.full((1, tokens), -1, jnp.int32)
        kvbuf[:, :, 0:LOW, :] = jnp.zeros((layers, groups, LOW, 2 * group), BF16)

    @pl.when(jnp.logical_not(has_next))
    def _():
        marks[1] = jnp.full((1, tokens), -1, jnp.int32)
        kvbuf[:, :, LOW + tokens :, :] = jnp.zeros((layers, groups, HIGH, 2 * group), BF16)

    span = min(256, head_width)

    def averager(size):
        head_row = lax.broadcasted_iota(jnp.int32, (size, size), 0) // HEAD_DIM
        head_col = lax.broadcasted_iota(jnp.int32, (size, size), 1) // HEAD_DIM
        return jnp.where(head_row == head_col, 1.0 / HEAD_DIM, 0.0).astype(BF16)

    def head_norm(raw, gain):
        weights = averager(raw.shape[1])
        squares = raw * raw
        coarse = squares.astype(BF16)
        fine = (squares - coarse.astype(F32)).astype(BF16)
        mean = jnp.dot(coarse, weights, preferred_element_type=F32) + jnp.dot(
            fine, weights, preferred_element_type=F32
        )
        repeats = raw.shape[1] // HEAD_DIM
        gain = gain if repeats == 1 else jnp.concatenate([gain] * repeats, axis=1)
        return (raw * lax.rsqrt(mean + EPS) * gain).astype(BF16)

    def build_tables():
        query_col = lax.broadcasted_iota(jnp.int32, (GRID_W, 128), 0)
        key_col = lax.rem(lax.broadcasted_iota(jnp.int32, (GRID_W, 128), 1), GRID_W)
        offset = key_col - query_col + WIN_COLS // 2
        band = (offset >= 0) & (offset < WIN_COLS)
        heads = head_width // HEAD_DIM
        tiles = KEYS // 128
        lines[...] = jnp.zeros_like(lines)
        for layer in range(layers):
            for head in range(heads):
                lines[:, 0:WIN_COLS] = bias_ref[layer, head]
                left = lines[...]
                right = pltpu.roll(left, GRID_W, 1)
                for tile in range(tiles):
                    j = 2 * tile
                    line = left[j : j + 1, :] + right[j + 1 : j + 2, :]
                    line = jnp.broadcast_to(line, (GRID_W, 128))
                    line = pltpu.roll(line, 128 - WIN_COLS // 2, 1, stride=1, stride_axis=0)
                    table[
                        layer,
                        head * GRID_W : (head + 1) * GRID_W,
                        tile * 128 : (tile + 1) * 128,
                    ] = jnp.where(band, line, NEG)

    def build_masks():
        own = doc_ref[...]
        every = jnp.concatenate([marks[0], own, marks[1]], axis=1).astype(F32)
        own_rows = jnp.broadcast_to(own.astype(F32), (128, tokens)).T
        base = tokens - LOW
        for row in range(rows):
            left = base + row * GRID_W
            keys_here = every[:, left : left + KEYS]
            queries_here = own_rows[row * GRID_W : (row + 1) * GRID_W, 0:1]
            maskbuf[row] = jnp.where(queries_here == keys_here, 0.0, NEG)

    lane = lax.broadcasted_iota(jnp.int32, (GRID_W, group), 1)

    def attend(layer, g, wanted):
        for row in wanted:
            low = row * GRID_W
            cols = slice(g * group, (g + 1) * group)
            q = qbuf[low : low + GRID_W, cols]
            if per_group == 2:
                zero = jnp.zeros_like(q)
                q = jnp.concatenate(
                    [
                        jnp.where(lane < HEAD_DIM, q, zero),
                        jnp.where(lane >= HEAD_DIM, q, zero),
                    ],
                    axis=0,
                )
            k = kvbuf[layer, g, low : low + KEYS, 0:group]
            v = kvbuf[layer, g, low : low + KEYS, group:]
            scores = lax.dot_general(
                q, k, (((1,), (1,)), ((), ())), preferred_element_type=F32
            )
            exps, sums = [], []
            for i in range(per_group):
                head = g * per_group + i
                s = (
                    scores[i * GRID_W : (i + 1) * GRID_W]
                    + table[layer, head * GRID_W : (head + 1) * GRID_W, :]
                    + maskbuf[row]
                )
                e = jnp.exp(s - jnp.max(s, axis=-1, keepdims=True))
                sums.append(jnp.sum(e, axis=-1, keepdims=True))
                exps.append(e.astype(BF16))
            weights = exps[0] if per_group == 1 else jnp.concatenate(exps, axis=0)
            mixed = jnp.dot(weights, v, preferred_element_type=F32)
            parts = [
                mixed[i * GRID_W : (i + 1) * GRID_W] / sums[i] for i in range(per_group)
            ]
            result = (
                parts[0] if per_group == 1 else jnp.where(lane < HEAD_DIM, parts[0], parts[1])
            )
            att[layer, mine, low : low + GRID_W, cols] = result.astype(BF16)

    chunk = 512
    for layer in range(layers):
        source = stream_ref if layer == 0 else hbuf
        target = out_ref if layer == layers - 1 else hbuf

        block = 32

        def norm_rows(i, carry):
            at = pl.ds(pl.multiple_of(i * block, block), block)
            x = source[at, :].astype(F32)
            inverse = lax.rsqrt(jnp.mean(x * x, axis=-1, keepdims=True) + EPS)
            nbuf[at, :] = (x * inverse * norm_gain_ref[layer : layer + 1, :]).astype(BF16)
            return carry

        lax.fori_loop(0, tokens // block, norm_rows, 0)

        k_gain = k_gain_ref[layer : layer + 1, :]
        q_gain = q_gain_ref[layer : layer + 1, :] * HEAD_DIM ** (-0.5)

        for g in range(groups):
            wkv_copy(layer, g, 0).wait()
            wkv_copy(layer, g, 1).wait()
            if layer == 0 and g == 0:
                wq_copy(0).start()
                wo_copy(0).start()
            own = slice(LOW, LOW + tokens)
            if paired:
                raw = jnp.dot(nbuf[...], wkvbuf[layer, g], preferred_element_type=F32)
                k_raw, v_raw = raw[:, 0:group], raw[:, group:]
            else:
                k_raw = jnp.dot(nbuf[...], wkvbuf[layer, 0], preferred_element_type=F32)
                v_raw = jnp.dot(nbuf[...], wkvbuf[layer, 1], preferred_element_type=F32)
            kvbuf[layer, g, own, 0:group] = head_norm(k_raw, k_gain)
            kvbuf[layer, g, own, group:] = v_raw.astype(BF16)
            if layer == 0 and g == 0:
                degree = has_prev.astype(jnp.int32) + has_next.astype(jnp.int32) + (tp_size - 1)
                pl.semaphore_wait(barrier, degree)
                start_both(mark_copies())
            start_both(halo(layer, g))

        if layer == 0:
            for later in range(1, layers):
                for g in range(groups):
                    wkv_copy(later, g, 0).start()
                    wkv_copy(later, g, 1).start()
                wq_copy(later).start()
                wo_copy(later).start()

        wq_copy(layer).wait()
        for start in range(0, head_width, span):
            cols = slice(start, start + span)
            raw = jnp.dot(nbuf[...], wqbuf[layer, :, cols], preferred_element_type=F32)
            qbuf[:, cols] = head_norm(raw, q_gain)
        if layer == 0:
            build_tables()
            wait_low(mark_copies())
            wait_high(mark_copies())
            build_masks()

        def attend_group(g):
            copies = halo(layer, g)
            wait_low(copies)
            attend(layer, g, range(0, 1))
            wait_high(copies)
            attend(layer, g, range(1, rows))
            for step in range(1, tp_size):
                att_copy(layer, g, step).start()

        def add_part(step, part, first, last):
            owner = lax.rem(mine + tp_size - step, tp_size)
            size = len(part) * group
            inner = slice(part[0] * group, part[0] * group + size)
            begin = owner * head_width + part[0] * group
            at = pl.ds(pl.multiple_of(begin, HEAD_DIM), size)
            if step > 0:
                for g in part:
                    att_copy(layer, g, step).wait_recv()
            for start in range(0, width, chunk):
                cols = slice(start, start + chunk)
                total = jnp.dot(
                    att[layer, owner, :, inner],
                    wobuf[layer, at, cols],
                    preferred_element_type=F32,
                )
                total += source[:, cols].astype(F32) if first else acc[:, cols]
                if last:
                    target[:, cols] = total.astype(BF16)
                else:
                    acc[:, cols] = total

        every = list(range(groups))
        half = groups // 2
        parts = [every[:half], every[half:]] if half else [every]
        pending = []
        for index, part in enumerate(parts):
            for g in part:
                attend_group(g)
                for job in pending:
                    add_part(*job)
                pending = []
            if index == 0:
                wo_copy(layer).wait()
            final = index == len(parts) - 1
            add_part(0, part, index == 0, final and tp_size == 1)
            pending = [
                (step, part, False, final and step == tp_size - 1)
                for step in range(1, tp_size)
            ]
        for job in pending:
            add_part(*job)

    wait_send_both(mark_copies())
    for layer in range(layers):
        for g in range(groups):
            wait_send_both(halo(layer, g))
            for step in range(1, tp_size):
                att_copy(layer, g, step).wait_send()


def on_device(
    sp_size,
    tp_size,
    stream,
    doc_ids,
    norm_gain,
    w_query,
    w_key,
    w_value,
    query_gain,
    key_gain,
    offset_bias,
    w_output,
):
    tokens, width = stream.shape
    layers, _, head_width = w_query.shape
    heads = head_width // HEAD_DIM
    rows = tokens // GRID_W
    all_width = w_output.shape[1]
    group = min(128, head_width)
    groups = head_width // group
    vmem = pl.BlockSpec(memory_space=pltpu.VMEM)
    hbm = pl.BlockSpec(memory_space=pl.ANY)
    sem = pltpu.SemaphoreType.DMA
    peers = max(1, tp_size - 1)
    return pl.pallas_call(
        functools.partial(kernel, sp_size, tp_size),
        out_shape=jax.ShapeDtypeStruct((tokens, width), BF16),
        in_specs=[vmem, vmem, vmem, hbm, hbm, hbm, vmem, vmem, vmem, hbm],
        out_specs=vmem,
        scratch_shapes=[
            pltpu.VMEM((layers, width, head_width), BF16),
            pltpu.VMEM(
                (layers, groups, width, 256) if group == 128 else (layers, 2, width, group), BF16
            ),
            pltpu.VMEM((layers, all_width, width), BF16),
            pltpu.VMEM((tokens, width), BF16),
            pltpu.VMEM((tokens, width), BF16),
            pltpu.VMEM((tokens, head_width), BF16),
            pltpu.VMEM((layers, groups, LOW + tokens + HIGH, 2 * group), BF16),
            pltpu.VMEM((layers, tp_size, tokens, head_width), BF16),
            pltpu.VMEM((tokens, width), F32),
            pltpu.VMEM((layers, heads * GRID_W, KEYS), F32),
            pltpu.VMEM((rows, GRID_W, KEYS), F32),
            pltpu.VMEM((2, 1, tokens), jnp.int32),
            pltpu.VMEM((WIN_ROWS, 128), F32),
            sem((layers,)),
            sem((layers, groups, 2)),
            sem((layers,)),
            sem((2,)),
            sem((2,)),
            sem((layers, groups, 2)),
            sem((layers, groups, 2)),
            sem((layers, peers, groups)),
            sem((layers, peers, groups)),
        ],
        compiler_params=pltpu.CompilerParams(
            collective_id=0, has_side_effects=True, vmem_limit_bytes=60 * 1024 * 1024
        ),
    )(
        stream,
        doc_ids.reshape(1, tokens),
        norm_gain,
        w_query,
        w_key,
        w_value,
        query_gain,
        key_gain,
        offset_bias,
        w_output,
    )


def solution(mesh):
    return jax.shard_map(
        functools.partial(on_device, mesh.shape["sp"], mesh.shape["tp"]),
        mesh=mesh,
        in_specs=(
            P("sp", None),
            P("sp"),
            P(),
            P(None, None, "tp"),
            P(None, None, "tp"),
            P(None, None, "tp"),
            P(),
            P(),
            P(None, "tp", None, None),
            P(),
        ),
        out_specs=P("sp", None),
        check_vma=False,
    )
```

```python
import functools

import jax
import jax.numpy as jnp
from jax import lax
from jax.experimental import pallas as pl
from jax.experimental.pallas import tpu as pltpu
from jax.sharding import PartitionSpec as P

HEAD_DIM = 64
GRID_W = 64
WIN_ROWS = 8
WIN_COLS = 16
EPS = 1e-06
LOW = WIN_ROWS // 2 * GRID_W
HIGH = (WIN_ROWS - WIN_ROWS // 2 - 1) * GRID_W
KEYS = WIN_ROWS * GRID_W
NEG = -1e30
MESH = pl.DeviceIdType.MESH
F32 = jnp.float32
BF16 = jnp.bfloat16


def kernel(
    sp_size,
    tp_size,
    stream_ref,
    doc_ref,
    norm_gain_ref,
    wq_hbm,
    wk_hbm,
    wv_hbm,
    q_gain_ref,
    k_gain_ref,
    bias_ref,
    wo_hbm,
    out_ref,
    wqbuf,
    wkvbuf,
    wobuf,
    hbuf,
    nbuf,
    qbuf,
    kvbuf,
    att,
    acc,
    table,
    maskbuf,
    marks,
    lines,
    wq_sem,
    wkv_sem,
    wo_sem,
    mark_send,
    mark_recv,
    kv_send,
    kv_recv,
    a_send,
    a_recv,
):
    layers, width, head_width = wk_hbm.shape
    tokens = stream_ref.shape[0]
    rows = tokens // GRID_W
    group = min(128, head_width)
    per_group = group // HEAD_DIM
    groups = head_width // group
    paired = group == 128
    me = lax.axis_index("sp")
    mine = lax.axis_index("tp")
    has_prev = me > 0
    has_next = me < sp_size - 1
    prev = lax.rem(me + sp_size - 1, sp_size)
    following = lax.rem(me + 1, sp_size)

    def wq_copy(layer):
        return pltpu.make_async_copy(wq_hbm.at[layer], wqbuf.at[layer], wq_sem.at[layer])

    def wkv_copy(layer, g, part):
        source = (wk_hbm, wv_hbm)[part].at[layer]
        if paired:
            source = source.at[:, pl.ds(g * group, group)]
            target = wkvbuf.at[layer, g, :, pl.ds(part * group, group)]
        else:
            target = wkvbuf.at[layer, part]
        return pltpu.make_async_copy(source, target, wkv_sem.at[layer, g, part])

    def wo_copy(layer):
        return pltpu.make_async_copy(wo_hbm.at[layer], wobuf.at[layer], wo_sem.at[layer])

    for g in range(groups):
        for part in range(2):
            wkv_copy(0, g, part).start()

    barrier = pltpu.get_barrier_semaphore()

    @pl.when(has_prev)
    def _():
        pl.semaphore_signal(barrier, inc=1, device_id={"sp": prev}, device_id_type=MESH)

    @pl.when(has_next)
    def _():
        pl.semaphore_signal(barrier, inc=1, device_id={"sp": following}, device_id_type=MESH)

    for step in range(1, tp_size):
        pl.semaphore_signal(
            barrier,
            inc=1,
            device_id={"tp": lax.rem(mine + step, tp_size)},
            device_id_type=MESH,
        )

    def halo(layer, g):
        here = kvbuf.at[layer, g]
        ahead = pltpu.make_async_remote_copy(
            src_ref=here.at[pl.ds(tokens, LOW)],
            dst_ref=here.at[pl.ds(0, LOW)],
            send_sem=kv_send.at[layer, g, 0],
            recv_sem=kv_recv.at[layer, g, 0],
            device_id={"sp": following},
            device_id_type=MESH,
        )
        back = pltpu.make_async_remote_copy(
            src_ref=here.at[pl.ds(LOW, HIGH)],
            dst_ref=here.at[pl.ds(LOW + tokens, HIGH)],
            send_sem=kv_send.at[layer, g, 1],
            recv_sem=kv_recv.at[layer, g, 1],
            device_id={"sp": prev},
            device_id_type=MESH,
        )
        return ahead, back

    def mark_copies():
        ahead = pltpu.make_async_remote_copy(
            src_ref=doc_ref,
            dst_ref=marks.at[0],
            send_sem=mark_send.at[0],
            recv_sem=mark_recv.at[0],
            device_id={"sp": following},
            device_id_type=MESH,
        )
        back = pltpu.make_async_remote_copy(
            src_ref=doc_ref,
            dst_ref=marks.at[1],
            send_sem=mark_send.at[1],
            recv_sem=mark_recv.at[1],
            device_id={"sp": prev},
            device_id_type=MESH,
        )
        return ahead, back

    def start_both(pair):
        @pl.when(has_next)
        def _():
            pair[0].start()

        @pl.when(has_prev)
        def _():
            pair[1].start()

    def wait_send_both(pair):
        @pl.when(has_next)
        def _():
            pair[0].wait_send()

        @pl.when(has_prev)
        def _():
            pair[1].wait_send()

    def wait_low(pair):
        @pl.when(has_prev)
        def _():
            pair[0].wait_recv()

    def wait_high(pair):
        @pl.when(has_next)
        def _():
            pair[1].wait_recv()

    def att_copy(layer, g, step):
        block = att.at[layer, mine, g]
        return pltpu.make_async_remote_copy(
            src_ref=block,
            dst_ref=block,
            send_sem=a_send.at[layer, step - 1, g],
            recv_sem=a_recv.at[layer, step - 1, g],
            device_id={"tp": lax.rem(mine + step, tp_size)},
            device_id_type=MESH,
        )

    @pl.when(jnp.logical_not(has_prev))
    def _():
        marks[0] = jnp.full((1, tokens), -1, jnp.int32)
        kvbuf[:, :, 0:LOW, :] = jnp.zeros((layers, groups, LOW, 2 * group), BF16)

    @pl.when(jnp.logical_not(has_next))
    def _():
        marks[1] = jnp.full((1, tokens), -1, jnp.int32)
        kvbuf[:, :, LOW + tokens :, :] = jnp.zeros((layers, groups, HIGH, 2 * group), BF16)

    span = min(256, head_width)

    def averager(size):
        head_row = lax.broadcasted_iota(jnp.int32, (size, size), 0) // HEAD_DIM
        head_col = lax.broadcasted_iota(jnp.int32, (size, size), 1) // HEAD_DIM
        return jnp.where(head_row == head_col, 1.0 / HEAD_DIM, 0.0).astype(BF16)

    def head_norm(raw, gain):
        weights = averager(raw.shape[1])
        squares = raw * raw
        coarse = squares.astype(BF16)
        fine = (squares - coarse.astype(F32)).astype(BF16)
        mean = jnp.dot(coarse, weights, preferred_element_type=F32) + jnp.dot(
            fine, weights, preferred_element_type=F32
        )
        repeats = raw.shape[1] // HEAD_DIM
        gain = gain if repeats == 1 else jnp.concatenate([gain] * repeats, axis=1)
        return (raw * lax.rsqrt(mean + EPS) * gain).astype(BF16)

    def build_tables():
        query_col = lax.broadcasted_iota(jnp.int32, (GRID_W, 128), 0)
        key_col = lax.rem(lax.broadcasted_iota(jnp.int32, (GRID_W, 128), 1), GRID_W)
        offset = key_col - query_col + WIN_COLS // 2
        band = (offset >= 0) & (offset < WIN_COLS)
        heads = head_width // HEAD_DIM
        tiles = KEYS // 128
        lines[...] = jnp.zeros_like(lines)
        for layer in range(layers):
            for head in range(heads):
                lines[:, 0:WIN_COLS] = bias_ref[layer, head]
                left = lines[...]
                right = pltpu.roll(left, GRID_W, 1)
                for tile in range(tiles):
                    j = 2 * tile
                    line = left[j : j + 1, :] + right[j + 1 : j + 2, :]
                    line = jnp.broadcast_to(line, (GRID_W, 128))
                    line = pltpu.roll(line, 128 - WIN_COLS // 2, 1, stride=1, stride_axis=0)
                    table[
                        layer,
                        head * GRID_W : (head + 1) * GRID_W,
                        tile * 128 : (tile + 1) * 128,
                    ] = jnp.where(band, line, NEG)

    def build_masks():
        own = doc_ref[...]
        every = jnp.concatenate([marks[0], own, marks[1]], axis=1).astype(F32)
        own_rows = jnp.broadcast_to(own.astype(F32), (128, tokens)).T
        base = tokens - LOW
        for row in range(rows):
            left = base + row * GRID_W
            keys_here = every[:, left : left + KEYS]
            queries_here = own_rows[row * GRID_W : (row + 1) * GRID_W, 0:1]
            maskbuf[row] = jnp.where(queries_here == keys_here, 0.0, NEG)

    lane = lax.broadcasted_iota(jnp.int32, (GRID_W, group), 1)

    def attend(layer, g, wanted):
        cols = slice(g * group, (g + 1) * group)
        scores, weights, sums = {}, {}, {}
        for row in wanted:
            low = row * GRID_W
            q = qbuf[low : low + GRID_W, cols]
            if per_group == 2:
                zero = jnp.zeros_like(q)
                q = jnp.concatenate(
                    [
                        jnp.where(lane < HEAD_DIM, q, zero),
                        jnp.where(lane >= HEAD_DIM, q, zero),
                    ],
                    axis=0,
                )
            k = kvbuf[layer, g, low : low + KEYS, 0:group]
            scores[row] = lax.dot_general(
                q, k, (((1,), (1,)), ((), ())), preferred_element_type=F32
            )
        for row in wanted:
            exps = []
            sums[row] = []
            for i in range(per_group):
                head = g * per_group + i
                s = (
                    scores[row][i * GRID_W : (i + 1) * GRID_W]
                    + table[layer, head * GRID_W : (head + 1) * GRID_W, :]
                    + maskbuf[row]
                )
                e = jnp.exp(s - jnp.max(s, axis=-1, keepdims=True))
                sums[row].append(jnp.sum(e, axis=-1, keepdims=True))
                exps.append(e.astype(BF16))
            weights[row] = exps[0] if per_group == 1 else jnp.concatenate(exps, axis=0)
        for row in wanted:
            low = row * GRID_W
            v = kvbuf[layer, g, low : low + KEYS, group:]
            mixed = jnp.dot(weights[row], v, preferred_element_type=F32)
            parts = [
                mixed[i * GRID_W : (i + 1) * GRID_W] / sums[row][i] for i in range(per_group)
            ]
            result = (
                parts[0] if per_group == 1 else jnp.where(lane < HEAD_DIM, parts[0], parts[1])
            )
            att[layer, mine, g, low : low + GRID_W, :] = result.astype(BF16)

    chunk = 512
    for layer in range(layers):
        source = stream_ref if layer == 0 else hbuf
        target = out_ref if layer == layers - 1 else hbuf

        block = 32

        def norm_rows(i, carry):
            at = pl.ds(pl.multiple_of(i * block, block), block)
            x = source[at, :].astype(F32)
            inverse = lax.rsqrt(jnp.mean(x * x, axis=-1, keepdims=True) + EPS)
            nbuf[at, :] = (x * inverse * norm_gain_ref[layer : layer + 1, :]).astype(BF16)
            return carry

        lax.fori_loop(0, tokens // block, norm_rows, 0)

        k_gain = k_gain_ref[layer : layer + 1, :]
        q_gain = q_gain_ref[layer : layer + 1, :] * HEAD_DIM ** (-0.5)

        for g in range(groups):
            wkv_copy(layer, g, 0).wait()
            wkv_copy(layer, g, 1).wait()
            if layer == 0 and g == 0:
                wq_copy(0).start()
                wo_copy(0).start()
            own = slice(LOW, LOW + tokens)
            if paired:
                raw = jnp.dot(nbuf[...], wkvbuf[layer, g], preferred_element_type=F32)
                k_raw, v_raw = raw[:, 0:group], raw[:, group:]
            else:
                k_raw = jnp.dot(nbuf[...], wkvbuf[layer, 0], preferred_element_type=F32)
                v_raw = jnp.dot(nbuf[...], wkvbuf[layer, 1], preferred_element_type=F32)
            kvbuf[layer, g, own, 0:group] = head_norm(k_raw, k_gain)
            kvbuf[layer, g, own, group:] = v_raw.astype(BF16)
            if layer == 0 and g == 0:
                degree = has_prev.astype(jnp.int32) + has_next.astype(jnp.int32) + (tp_size - 1)
                pl.semaphore_wait(barrier, degree)
                start_both(mark_copies())
            start_both(halo(layer, g))

        if layer == 0:
            for later in range(1, layers):
                for g in range(groups):
                    wkv_copy(later, g, 0).start()
                    wkv_copy(later, g, 1).start()
                wq_copy(later).start()
                wo_copy(later).start()

        wq_copy(layer).wait()
        for start in range(0, head_width, span):
            cols = slice(start, start + span)
            raw = jnp.dot(nbuf[...], wqbuf[layer, :, cols], preferred_element_type=F32)
            qbuf[:, cols] = head_norm(raw, q_gain)
        if layer == 0:
            build_tables()
            wait_low(mark_copies())
            wait_high(mark_copies())
            build_masks()

        def attend_group(g):
            copies = halo(layer, g)
            wait_low(copies)
            wait_high(copies)
            attend(layer, g, range(rows))
            for step in range(1, tp_size):
                att_copy(layer, g, step).start()

        def add_part(step, part, first, last):
            owner = lax.rem(mine + tp_size - step, tp_size)
            size = len(part) * group
            begin = owner * head_width + part[0] * group
            at = pl.ds(pl.multiple_of(begin, HEAD_DIM), size)
            if step > 0:
                for g in part:
                    att_copy(layer, g, step).wait_recv()
            pieces = [att[layer, owner, g] for g in part]
            heads_in = pieces[0] if len(pieces) == 1 else jnp.concatenate(pieces, axis=1)
            for start in range(0, width, chunk):
                cols = slice(start, start + chunk)
                total = jnp.dot(
                    heads_in,
                    wobuf[layer, at, cols],
                    preferred_element_type=F32,
                )
                total += source[:, cols].astype(F32) if first else acc[:, cols]
                if last:
                    target[:, cols] = total.astype(BF16)
                else:
                    acc[:, cols] = total

        every = list(range(groups))
        half = groups // 2
        parts = [every[:half], every[half:]] if half else [every]
        pending = []
        for index, part in enumerate(parts):
            for g in part:
                attend_group(g)
                for job in pending:
                    add_part(*job)
                pending = []
            if index == 0:
                wo_copy(layer).wait()
            final = index == len(parts) - 1
            add_part(0, part, index == 0, final and tp_size == 1)
            pending = [
                (step, part, False, final and step == tp_size - 1)
                for step in range(1, tp_size)
            ]
        for job in pending:
            add_part(*job)

    wait_send_both(mark_copies())
    for layer in range(layers):
        for g in range(groups):
            wait_send_both(halo(layer, g))
            for step in range(1, tp_size):
                att_copy(layer, g, step).wait_send()


def on_device(
    sp_size,
    tp_size,
    stream,
    doc_ids,
    norm_gain,
    w_query,
    w_key,
    w_value,
    query_gain,
    key_gain,
    offset_bias,
    w_output,
):
    tokens, width = stream.shape
    layers, _, head_width = w_query.shape
    heads = head_width // HEAD_DIM
    rows = tokens // GRID_W
    all_width = w_output.shape[1]
    group = min(128, head_width)
    groups = head_width // group
    vmem = pl.BlockSpec(memory_space=pltpu.VMEM)
    hbm = pl.BlockSpec(memory_space=pl.ANY)
    sem = pltpu.SemaphoreType.DMA
    peers = max(1, tp_size - 1)
    return pl.pallas_call(
        functools.partial(kernel, sp_size, tp_size),
        out_shape=jax.ShapeDtypeStruct((tokens, width), BF16),
        in_specs=[vmem, vmem, vmem, hbm, hbm, hbm, vmem, vmem, vmem, hbm],
        out_specs=vmem,
        scratch_shapes=[
            pltpu.VMEM((layers, width, head_width), BF16),
            pltpu.VMEM(
                (layers, groups, width, 256) if group == 128 else (layers, 2, width, group), BF16
            ),
            pltpu.VMEM((layers, all_width, width), BF16),
            pltpu.VMEM((tokens, width), BF16),
            pltpu.VMEM((tokens, width), BF16),
            pltpu.VMEM((tokens, head_width), BF16),
            pltpu.VMEM((layers, groups, LOW + tokens + HIGH, 2 * group), BF16),
            pltpu.VMEM((layers, tp_size, groups, tokens, group), BF16),
            pltpu.VMEM((tokens, width), F32),
            pltpu.VMEM((layers, heads * GRID_W, KEYS), F32),
            pltpu.VMEM((rows, GRID_W, KEYS), F32),
            pltpu.VMEM((2, 1, tokens), jnp.int32),
            pltpu.VMEM((WIN_ROWS, 128), F32),
            sem((layers,)),
            sem((layers, groups, 2)),
            sem((layers,)),
            sem((2,)),
            sem((2,)),
            sem((layers, groups, 2)),
            sem((layers, groups, 2)),
            sem((layers, peers, groups)),
            sem((layers, peers, groups)),
        ],
        compiler_params=pltpu.CompilerParams(
            collective_id=0, has_side_effects=True, vmem_limit_bytes=60 * 1024 * 1024
        ),
    )(
        stream,
        doc_ids.reshape(1, tokens),
        norm_gain,
        w_query,
        w_key,
        w_value,
        query_gain,
        key_gain,
        offset_bias,
        w_output,
    )


def solution(mesh):
    return jax.shard_map(
        functools.partial(on_device, mesh.shape["sp"], mesh.shape["tp"]),
        mesh=mesh,
        in_specs=(
            P("sp", None),
            P("sp"),
            P(),
            P(None, None, "tp"),
            P(None, None, "tp"),
            P(None, None, "tp"),
            P(),
            P(),
            P(None, "tp", None, None),
            P(),
        ),
        out_specs=P("sp", None),
        check_vma=False,
    )
```

```python
import functools

import jax
import jax.numpy as jnp
from jax import lax
from jax.experimental import pallas as pl
from jax.experimental.pallas import tpu as pltpu
from jax.sharding import PartitionSpec as P

HEAD_DIM = 64
GRID_W = 64
WIN_ROWS = 8
WIN_COLS = 16
EPS = 1e-06
LOW = WIN_ROWS // 2 * GRID_W
HIGH = (WIN_ROWS - WIN_ROWS // 2 - 1) * GRID_W
KEYS = WIN_ROWS * GRID_W
NEG = -1e30
CHUNK = 512
MESH = pl.DeviceIdType.MESH
F32 = jnp.float32
BF16 = jnp.bfloat16


def kernel(
    sp_size,
    tp_size,
    stream_ref,
    doc_ref,
    norm_gain_ref,
    wq_hbm,
    wk_hbm,
    wv_hbm,
    q_gain_ref,
    k_gain_ref,
    bias_ref,
    wo_hbm,
    out_ref,
    wqbuf,
    wkvbuf,
    wobuf,
    hbuf,
    nbuf,
    qbuf,
    kvbuf,
    att,
    acc,
    table,
    maskbuf,
    marks,
    lines,
    wq_sem,
    wkv_sem,
    wo_sem,
    mark_send,
    mark_recv,
    kv_send,
    kv_recv,
    a_send,
    a_recv,
    out_sem,
):
    layers, width, head_width = wk_hbm.shape
    tokens = stream_ref.shape[0]
    rows = tokens // GRID_W
    group = min(128, head_width)
    per_group = group // HEAD_DIM
    groups = head_width // group
    paired = group == 128
    me = lax.axis_index("sp")
    mine = lax.axis_index("tp")
    has_prev = me > 0
    has_next = me < sp_size - 1
    prev = lax.rem(me + sp_size - 1, sp_size)
    following = lax.rem(me + 1, sp_size)

    def wq_copy(layer):
        return pltpu.make_async_copy(wq_hbm.at[layer], wqbuf.at[layer], wq_sem.at[layer])

    def wkv_copy(layer, g, part):
        source = (wk_hbm, wv_hbm)[part].at[layer]
        if paired:
            source = source.at[:, pl.ds(g * group, group)]
            target = wkvbuf.at[layer, g, :, pl.ds(part * group, group)]
        else:
            target = wkvbuf.at[layer, part]
        return pltpu.make_async_copy(source, target, wkv_sem.at[layer, g, part])

    def wo_copy(layer):
        return pltpu.make_async_copy(wo_hbm.at[layer], wobuf.at[layer], wo_sem.at[layer])

    for g in range(groups):
        for part in range(2):
            wkv_copy(0, g, part).start()

    barrier = pltpu.get_barrier_semaphore()

    @pl.when(has_prev)
    def _():
        pl.semaphore_signal(barrier, inc=1, device_id={"sp": prev}, device_id_type=MESH)

    @pl.when(has_next)
    def _():
        pl.semaphore_signal(barrier, inc=1, device_id={"sp": following}, device_id_type=MESH)

    for step in range(1, tp_size):
        pl.semaphore_signal(
            barrier,
            inc=1,
            device_id={"tp": lax.rem(mine + step, tp_size)},
            device_id_type=MESH,
        )

    def pieces_of(g):
        return 2 if g == groups - 1 and rows % 2 == 0 else 1

    def halo(layer, g):
        here = kvbuf.at[layer, g]
        ahead = pltpu.make_async_remote_copy(
            src_ref=here.at[pl.ds(tokens, LOW)],
            dst_ref=here.at[pl.ds(0, LOW)],
            send_sem=kv_send.at[layer, g, 0],
            recv_sem=kv_recv.at[layer, g, 0],
            device_id={"sp": following},
            device_id_type=MESH,
        )
        back = pltpu.make_async_remote_copy(
            src_ref=here.at[pl.ds(LOW, HIGH)],
            dst_ref=here.at[pl.ds(LOW + tokens, HIGH)],
            send_sem=kv_send.at[layer, g, 1],
            recv_sem=kv_recv.at[layer, g, 1],
            device_id={"sp": prev},
            device_id_type=MESH,
        )
        return ahead, back

    def mark_copies():
        ahead = pltpu.make_async_remote_copy(
            src_ref=doc_ref,
            dst_ref=marks.at[0],
            send_sem=mark_send.at[0],
            recv_sem=mark_recv.at[0],
            device_id={"sp": following},
            device_id_type=MESH,
        )
        back = pltpu.make_async_remote_copy(
            src_ref=doc_ref,
            dst_ref=marks.at[1],
            send_sem=mark_send.at[1],
            recv_sem=mark_recv.at[1],
            device_id={"sp": prev},
            device_id_type=MESH,
        )
        return ahead, back

    def start_both(pair):
        @pl.when(has_next)
        def _():
            pair[0].start()

        @pl.when(has_prev)
        def _():
            pair[1].start()

    def wait_send_both(pair):
        @pl.when(has_next)
        def _():
            pair[0].wait_send()

        @pl.when(has_prev)
        def _():
            pair[1].wait_send()

    def wait_low(pair):
        @pl.when(has_prev)
        def _():
            pair[0].wait_recv()

    def wait_high(pair):
        @pl.when(has_next)
        def _():
            pair[1].wait_recv()

    def att_copy(layer, g, step, piece):
        if pieces_of(g) == 1:
            block = att.at[layer, mine, g]
        else:
            block = att.at[layer, mine, g, pl.ds(piece * (tokens // 2), tokens // 2)]
        return pltpu.make_async_remote_copy(
            src_ref=block,
            dst_ref=block,
            send_sem=a_send.at[layer, step - 1, g, piece],
            recv_sem=a_recv.at[layer, step - 1, g, piece],
            device_id={"tp": lax.rem(mine + step, tp_size)},
            device_id_type=MESH,
        )

    @pl.when(jnp.logical_not(has_prev))
    def _():
        marks[0] = jnp.full((1, tokens), -1, jnp.int32)
        kvbuf[:, :, 0:LOW, :] = jnp.zeros((layers, groups, LOW, 2 * group), BF16)

    @pl.when(jnp.logical_not(has_next))
    def _():
        marks[1] = jnp.full((1, tokens), -1, jnp.int32)
        kvbuf[:, :, LOW + tokens :, :] = jnp.zeros((layers, groups, HIGH, 2 * group), BF16)

    span = min(256, head_width)

    def averager(size):
        head_row = lax.broadcasted_iota(jnp.int32, (size, size), 0) // HEAD_DIM
        head_col = lax.broadcasted_iota(jnp.int32, (size, size), 1) // HEAD_DIM
        return jnp.where(head_row == head_col, 1.0 / HEAD_DIM, 0.0).astype(BF16)

    def head_norm(raw, gain):
        weights = averager(raw.shape[1])
        squares = raw * raw
        coarse = squares.astype(BF16)
        fine = (squares - coarse.astype(F32)).astype(BF16)
        mean = jnp.dot(coarse, weights, preferred_element_type=F32) + jnp.dot(
            fine, weights, preferred_element_type=F32
        )
        repeats = raw.shape[1] // HEAD_DIM
        gain = gain if repeats == 1 else jnp.concatenate([gain] * repeats, axis=1)
        return (raw * lax.rsqrt(mean + EPS) * gain).astype(BF16)

    def build_tables():
        query_col = lax.broadcasted_iota(jnp.int32, (GRID_W, 128), 0)
        key_col = lax.rem(lax.broadcasted_iota(jnp.int32, (GRID_W, 128), 1), GRID_W)
        offset = key_col - query_col + WIN_COLS // 2
        band = (offset >= 0) & (offset < WIN_COLS)
        heads = head_width // HEAD_DIM
        tiles = KEYS // 128
        lines[...] = jnp.zeros_like(lines)
        for layer in range(layers):
            for head in range(heads):
                lines[:, 0:WIN_COLS] = bias_ref[layer, head]
                left = lines[...]
                right = pltpu.roll(left, GRID_W, 1)
                for tile in range(tiles):
                    j = 2 * tile
                    line = left[j : j + 1, :] + right[j + 1 : j + 2, :]
                    line = jnp.broadcast_to(line, (GRID_W, 128))
                    line = pltpu.roll(line, 128 - WIN_COLS // 2, 1, stride=1, stride_axis=0)
                    table[
                        layer,
                        head * GRID_W : (head + 1) * GRID_W,
                        tile * 128 : (tile + 1) * 128,
                    ] = jnp.where(band, line, NEG)

    def build_masks():
        own = doc_ref[...]
        every = jnp.concatenate([marks[0], own, marks[1]], axis=1).astype(F32)
        own_rows = jnp.broadcast_to(own.astype(F32), (128, tokens)).T
        base = tokens - LOW
        for row in range(rows):
            left = base + row * GRID_W
            keys_here = every[:, left : left + KEYS]
            queries_here = own_rows[row * GRID_W : (row + 1) * GRID_W, 0:1]
            maskbuf[row] = jnp.where(queries_here == keys_here, 0.0, NEG)

    lane = lax.broadcasted_iota(jnp.int32, (GRID_W, group), 1)

    def out_copy(index):
        cols = pl.ds(index * CHUNK, CHUNK)
        return pltpu.make_async_copy(hbuf.at[:, cols], out_ref.at[:, cols], out_sem.at[index])

    def attend(layer, g, wanted):
        cols = slice(g * group, (g + 1) * group)
        scores, weights, sums = {}, {}, {}
        for row in wanted:
            low = row * GRID_W
            q = qbuf[low : low + GRID_W, cols]
            if per_group == 2:
                zero = jnp.zeros_like(q)
                q = jnp.concatenate(
                    [
                        jnp.where(lane < HEAD_DIM, q, zero),
                        jnp.where(lane >= HEAD_DIM, q, zero),
                    ],
                    axis=0,
                )
            k = kvbuf[layer, g, low : low + KEYS, 0:group]
            scores[row] = lax.dot_general(
                q, k, (((1,), (1,)), ((), ())), preferred_element_type=F32
            )
        for row in wanted:
            exps = []
            sums[row] = []
            for i in range(per_group):
                head = g * per_group + i
                s = (
                    scores[row][i * GRID_W : (i + 1) * GRID_W]
                    + table[layer, head * GRID_W : (head + 1) * GRID_W, :]
                    + maskbuf[row]
                )
                e = jnp.exp(s - jnp.max(s, axis=-1, keepdims=True))
                sums[row].append(jnp.sum(e, axis=-1, keepdims=True))
                exps.append(e.astype(BF16))
            weights[row] = exps[0] if per_group == 1 else jnp.concatenate(exps, axis=0)
        for row in wanted:
            low = row * GRID_W
            v = kvbuf[layer, g, low : low + KEYS, group:]
            mixed = jnp.dot(weights[row], v, preferred_element_type=F32)
            parts = [
                mixed[i * GRID_W : (i + 1) * GRID_W] / sums[row][i] for i in range(per_group)
            ]
            result = (
                parts[0] if per_group == 1 else jnp.where(lane < HEAD_DIM, parts[0], parts[1])
            )
            att[layer, mine, g, low : low + GRID_W, :] = result.astype(BF16)

    chunk = CHUNK
    for layer in range(layers):
        source = stream_ref if layer == 0 else hbuf

        block = 32

        def norm_rows(i, carry):
            at = pl.ds(pl.multiple_of(i * block, block), block)
            x = source[at, :].astype(F32)
            inverse = lax.rsqrt(jnp.mean(x * x, axis=-1, keepdims=True) + EPS)
            nbuf[at, :] = (x * inverse * norm_gain_ref[layer : layer + 1, :]).astype(BF16)
            return carry

        lax.fori_loop(0, tokens // block, norm_rows, 0)

        k_gain = k_gain_ref[layer : layer + 1, :]
        q_gain = q_gain_ref[layer : layer + 1, :] * HEAD_DIM ** (-0.5)

        for g in range(groups):
            wkv_copy(layer, g, 0).wait()
            wkv_copy(layer, g, 1).wait()
            if layer == 0 and g == 0:
                wq_copy(0).start()
                wo_copy(0).start()
            own = slice(LOW, LOW + tokens)
            if paired:
                raw = jnp.dot(nbuf[...], wkvbuf[layer, g], preferred_element_type=F32)
                k_raw, v_raw = raw[:, 0:group], raw[:, group:]
            else:
                k_raw = jnp.dot(nbuf[...], wkvbuf[layer, 0], preferred_element_type=F32)
                v_raw = jnp.dot(nbuf[...], wkvbuf[layer, 1], preferred_element_type=F32)
            kvbuf[layer, g, own, 0:group] = head_norm(k_raw, k_gain)
            kvbuf[layer, g, own, group:] = v_raw.astype(BF16)
            if layer == 0 and g == 0:
                degree = has_prev.astype(jnp.int32) + has_next.astype(jnp.int32) + (tp_size - 1)
                pl.semaphore_wait(barrier, degree)
                start_both(mark_copies())
            start_both(halo(layer, g))

        if layer == 0:
            for later in range(1, layers):
                for g in range(groups):
                    wkv_copy(later, g, 0).start()
                    wkv_copy(later, g, 1).start()
                wq_copy(later).start()
                wo_copy(later).start()

        wq_copy(layer).wait()
        for start in range(0, head_width, span):
            cols = slice(start, start + span)
            raw = jnp.dot(nbuf[...], wqbuf[layer, :, cols], preferred_element_type=F32)
            qbuf[:, cols] = head_norm(raw, q_gain)
        if layer == 0:
            build_tables()
            wait_low(mark_copies())
            wait_high(mark_copies())
            build_masks()

        def attend_group(g):
            copies = halo(layer, g)
            wait_low(copies)
            wait_high(copies)
            count = rows // pieces_of(g)
            for piece in range(pieces_of(g)):
                attend(layer, g, range(piece * count, (piece + 1) * count))
                for step in range(1, tp_size):
                    att_copy(layer, g, step, piece).start()

        def add_part(step, part, first, last):
            owner = lax.rem(mine + tp_size - step, tp_size)
            size = len(part) * group
            begin = owner * head_width + part[0] * group
            at = pl.ds(pl.multiple_of(begin, HEAD_DIM), size)
            if step > 0:
                for g in part:
                    for piece in range(pieces_of(g)):
                        att_copy(layer, g, step, piece).wait_recv()
            pieces = [att[layer, owner, g] for g in part]
            heads_in = pieces[0] if len(pieces) == 1 else jnp.concatenate(pieces, axis=1)
            for start in range(0, width, chunk):
                cols = slice(start, start + chunk)
                total = jnp.dot(
                    heads_in,
                    wobuf[layer, at, cols],
                    preferred_element_type=F32,
                )
                total += source[:, cols].astype(F32) if first else acc[:, cols]
                if last:
                    hbuf[:, cols] = total.astype(BF16)
                    if layer == layers - 1 and start > 0:
                        out_copy(start // chunk - 1).start()
                else:
                    acc[:, cols] = total

        every = list(range(groups))
        half = groups // 2
        parts = [every[:half], every[half:]] if half else [every]
        pending = []
        for index, part in enumerate(parts):
            for g in part:
                attend_group(g)
                for job in pending:
                    add_part(*job)
                pending = []
            if index == 0:
                wo_copy(layer).wait()
            final = index == len(parts) - 1
            add_part(0, part, index == 0, final and tp_size == 1)
            pending = [
                (step, part, False, final and step == tp_size - 1)
                for step in range(1, tp_size)
            ]
        for job in pending:
            add_part(*job)

    out_copy(width // chunk - 1).start()
    wait_send_both(mark_copies())
    for layer in range(layers):
        for g in range(groups):
            wait_send_both(halo(layer, g))
            for step in range(1, tp_size):
                for piece in range(pieces_of(g)):
                    att_copy(layer, g, step, piece).wait_send()
    for index in range(width // CHUNK):
        out_copy(index).wait()


def on_device(
    sp_size,
    tp_size,
    stream,
    doc_ids,
    norm_gain,
    w_query,
    w_key,
    w_value,
    query_gain,
    key_gain,
    offset_bias,
    w_output,
):
    tokens, width = stream.shape
    layers, _, head_width = w_query.shape
    heads = head_width // HEAD_DIM
    rows = tokens // GRID_W
    all_width = w_output.shape[1]
    group = min(128, head_width)
    groups = head_width // group
    vmem = pl.BlockSpec(memory_space=pltpu.VMEM)
    hbm = pl.BlockSpec(memory_space=pl.ANY)
    sem = pltpu.SemaphoreType.DMA
    peers = max(1, tp_size - 1)
    return pl.pallas_call(
        functools.partial(kernel, sp_size, tp_size),
        out_shape=jax.ShapeDtypeStruct((tokens, width), BF16),
        in_specs=[vmem, vmem, vmem, hbm, hbm, hbm, vmem, vmem, vmem, hbm],
        out_specs=hbm,
        scratch_shapes=[
            pltpu.VMEM((layers, width, head_width), BF16),
            pltpu.VMEM(
                (layers, groups, width, 256) if group == 128 else (layers, 2, width, group), BF16
            ),
            pltpu.VMEM((layers, all_width, width), BF16),
            pltpu.VMEM((tokens, width), BF16),
            pltpu.VMEM((tokens, width), BF16),
            pltpu.VMEM((tokens, head_width), BF16),
            pltpu.VMEM((layers, groups, LOW + tokens + HIGH, 2 * group), BF16),
            pltpu.VMEM((layers, tp_size, groups, tokens, group), BF16),
            pltpu.VMEM((tokens, width), F32),
            pltpu.VMEM((layers, heads * GRID_W, KEYS), F32),
            pltpu.VMEM((rows, GRID_W, KEYS), F32),
            pltpu.VMEM((2, 1, tokens), jnp.int32),
            pltpu.VMEM((WIN_ROWS, 128), F32),
            sem((layers,)),
            sem((layers, groups, 2)),
            sem((layers,)),
            sem((2,)),
            sem((2,)),
            sem((layers, groups, 2)),
            sem((layers, groups, 2)),
            sem((layers, peers, groups, 2)),
            sem((layers, peers, groups, 2)),
            sem((width // CHUNK,)),
        ],
        compiler_params=pltpu.CompilerParams(
            collective_id=0, has_side_effects=True, vmem_limit_bytes=60 * 1024 * 1024
        ),
    )(
        stream,
        doc_ids.reshape(1, tokens),
        norm_gain,
        w_query,
        w_key,
        w_value,
        query_gain,
        key_gain,
        offset_bias,
        w_output,
    )


def solution(mesh):
    return jax.shard_map(
        functools.partial(on_device, mesh.shape["sp"], mesh.shape["tp"]),
        mesh=mesh,
        in_specs=(
            P("sp", None),
            P("sp"),
            P(),
            P(None, None, "tp"),
            P(None, None, "tp"),
            P(None, None, "tp"),
            P(),
            P(),
            P(None, "tp", None, None),
            P(),
        ),
        out_specs=P("sp", None),
        check_vma=False,
    )
```

```python
import functools

import jax
import jax.numpy as jnp
from jax import lax
from jax.experimental import pallas as pl
from jax.experimental.pallas import tpu as pltpu
from jax.sharding import PartitionSpec as P

HEAD_DIM = 64
GRID_W = 64
WIN_ROWS = 8
WIN_COLS = 16
EPS = 1e-06
LOW = WIN_ROWS // 2 * GRID_W
HIGH = (WIN_ROWS - WIN_ROWS // 2 - 1) * GRID_W
KEYS = WIN_ROWS * GRID_W
NEG = -1e30
CHUNK = 512
MESH = pl.DeviceIdType.MESH
F32 = jnp.float32
BF16 = jnp.bfloat16


def kernel(
    sp_size,
    tp_size,
    stream_ref,
    doc_ref,
    norm_gain_ref,
    wq_hbm,
    wk_hbm,
    wv_hbm,
    q_gain_ref,
    k_gain_ref,
    bias_ref,
    wo_hbm,
    out_ref,
    wqbuf,
    wkvbuf,
    wobuf,
    hbuf,
    nbuf,
    qbuf,
    kvbuf,
    att,
    acc,
    table,
    maskbuf,
    marks,
    lines,
    wq_sem,
    wkv_sem,
    wo_sem,
    mark_send,
    mark_recv,
    kv_send,
    kv_recv,
    a_send,
    a_recv,
    out_sem,
):
    layers, width, head_width = wk_hbm.shape
    tokens = stream_ref.shape[0]
    rows = tokens // GRID_W
    group = min(128, head_width)
    per_group = group // HEAD_DIM
    groups = head_width // group
    paired = group == 128
    me = lax.axis_index("sp")
    mine = lax.axis_index("tp")
    has_prev = me > 0
    has_next = me < sp_size - 1
    prev = lax.rem(me + sp_size - 1, sp_size)
    following = lax.rem(me + 1, sp_size)

    def wq_copy(layer):
        return pltpu.make_async_copy(wq_hbm.at[layer], wqbuf.at[layer], wq_sem.at[layer])

    def wkv_copy(layer, g, part):
        source = (wk_hbm, wv_hbm)[part].at[layer]
        if paired:
            source = source.at[:, pl.ds(g * group, group)]
            target = wkvbuf.at[layer, g, :, pl.ds(part * group, group)]
        else:
            target = wkvbuf.at[layer, part]
        return pltpu.make_async_copy(source, target, wkv_sem.at[layer, g, part])

    def wo_copy(layer):
        return pltpu.make_async_copy(wo_hbm.at[layer], wobuf.at[layer], wo_sem.at[layer])

    for g in range(groups):
        for part in range(2):
            wkv_copy(0, g, part).start()

    barrier = pltpu.get_barrier_semaphore()

    @pl.when(has_prev)
    def _():
        pl.semaphore_signal(barrier, inc=1, device_id={"sp": prev}, device_id_type=MESH)

    @pl.when(has_next)
    def _():
        pl.semaphore_signal(barrier, inc=1, device_id={"sp": following}, device_id_type=MESH)

    for step in range(1, tp_size):
        pl.semaphore_signal(
            barrier,
            inc=1,
            device_id={"tp": lax.rem(mine + step, tp_size)},
            device_id_type=MESH,
        )

    def pieces_of(g):
        return 2 if g == groups - 1 and rows % 2 == 0 else 1

    def halo(layer, g):
        here = kvbuf.at[layer, g]
        ahead = pltpu.make_async_remote_copy(
            src_ref=here.at[pl.ds(tokens, LOW)],
            dst_ref=here.at[pl.ds(0, LOW)],
            send_sem=kv_send.at[layer, g, 0],
            recv_sem=kv_recv.at[layer, g, 0],
            device_id={"sp": following},
            device_id_type=MESH,
        )
        back = pltpu.make_async_remote_copy(
            src_ref=here.at[pl.ds(LOW, HIGH)],
            dst_ref=here.at[pl.ds(LOW + tokens, HIGH)],
            send_sem=kv_send.at[layer, g, 1],
            recv_sem=kv_recv.at[layer, g, 1],
            device_id={"sp": prev},
            device_id_type=MESH,
        )
        return ahead, back

    def mark_copies():
        ahead = pltpu.make_async_remote_copy(
            src_ref=doc_ref,
            dst_ref=marks.at[0],
            send_sem=mark_send.at[0],
            recv_sem=mark_recv.at[0],
            device_id={"sp": following},
            device_id_type=MESH,
        )
        back = pltpu.make_async_remote_copy(
            src_ref=doc_ref,
            dst_ref=marks.at[1],
            send_sem=mark_send.at[1],
            recv_sem=mark_recv.at[1],
            device_id={"sp": prev},
            device_id_type=MESH,
        )
        return ahead, back

    def start_both(pair):
        @pl.when(has_next)
        def _():
            pair[0].start()

        @pl.when(has_prev)
        def _():
            pair[1].start()

    def wait_send_both(pair):
        @pl.when(has_next)
        def _():
            pair[0].wait_send()

        @pl.when(has_prev)
        def _():
            pair[1].wait_send()

    def wait_low(pair):
        @pl.when(has_prev)
        def _():
            pair[0].wait_recv()

    def wait_high(pair):
        @pl.when(has_next)
        def _():
            pair[1].wait_recv()

    def att_copy(layer, g, step, piece):
        if pieces_of(g) == 1:
            block = att.at[layer, mine, g]
        else:
            block = att.at[layer, mine, g, pl.ds(piece * (tokens // 2), tokens // 2)]
        return pltpu.make_async_remote_copy(
            src_ref=block,
            dst_ref=block,
            send_sem=a_send.at[layer, step - 1, g, piece],
            recv_sem=a_recv.at[layer, step - 1, g, piece],
            device_id={"tp": lax.rem(mine + step, tp_size)},
            device_id_type=MESH,
        )

    @pl.when(jnp.logical_not(has_prev))
    def _():
        marks[0] = jnp.full((1, tokens), -1, jnp.int32)
        kvbuf[:, :, 0:LOW, :] = jnp.zeros((layers, groups, LOW, 2 * group), BF16)

    @pl.when(jnp.logical_not(has_next))
    def _():
        marks[1] = jnp.full((1, tokens), -1, jnp.int32)
        kvbuf[:, :, LOW + tokens :, :] = jnp.zeros((layers, groups, HIGH, 2 * group), BF16)

    span = min(256, head_width)

    def averager(size):
        head_row = lax.broadcasted_iota(jnp.int32, (size, size), 0) // HEAD_DIM
        head_col = lax.broadcasted_iota(jnp.int32, (size, size), 1) // HEAD_DIM
        return jnp.where(head_row == head_col, 1.0 / HEAD_DIM, 0.0).astype(BF16)

    def head_norm(raw, gain):
        weights = averager(raw.shape[1])
        squares = raw * raw
        coarse = squares.astype(BF16)
        fine = (squares - coarse.astype(F32)).astype(BF16)
        mean = jnp.dot(coarse, weights, preferred_element_type=F32) + jnp.dot(
            fine, weights, preferred_element_type=F32
        )
        repeats = raw.shape[1] // HEAD_DIM
        gain = gain if repeats == 1 else jnp.concatenate([gain] * repeats, axis=1)
        return (raw * lax.rsqrt(mean + EPS) * gain).astype(BF16)

    def build_tables():
        query_col = lax.broadcasted_iota(jnp.int32, (GRID_W, 128), 0)
        key_col = lax.rem(lax.broadcasted_iota(jnp.int32, (GRID_W, 128), 1), GRID_W)
        offset = key_col - query_col + WIN_COLS // 2
        band = (offset >= 0) & (offset < WIN_COLS)
        heads = head_width // HEAD_DIM
        tiles = KEYS // 128
        lines[...] = jnp.zeros_like(lines)
        for layer in range(layers):
            for head in range(heads):
                lines[:, 0:WIN_COLS] = bias_ref[layer, head]
                left = lines[...]
                right = pltpu.roll(left, GRID_W, 1)
                for tile in range(tiles):
                    j = 2 * tile
                    line = left[j : j + 1, :] + right[j + 1 : j + 2, :]
                    line = jnp.broadcast_to(line, (GRID_W, 128))
                    line = pltpu.roll(line, 128 - WIN_COLS // 2, 1, stride=1, stride_axis=0)
                    table[
                        layer,
                        head * GRID_W : (head + 1) * GRID_W,
                        tile * 128 : (tile + 1) * 128,
                    ] = jnp.where(band, line, NEG)

    def build_masks():
        own = doc_ref[...]
        every = jnp.concatenate([marks[0], own, marks[1]], axis=1).astype(F32)
        own_rows = jnp.broadcast_to(own.astype(F32), (128, tokens)).T
        base = tokens - LOW
        for row in range(rows):
            left = base + row * GRID_W
            keys_here = every[:, left : left + KEYS]
            queries_here = own_rows[row * GRID_W : (row + 1) * GRID_W, 0:1]
            maskbuf[row] = jnp.where(queries_here == keys_here, 0.0, NEG)

    lane = lax.broadcasted_iota(jnp.int32, (GRID_W, group), 1)

    def out_copy(index):
        cols = pl.ds(index * CHUNK, CHUNK)
        return pltpu.make_async_copy(hbuf.at[:, cols], out_ref.at[:, cols], out_sem.at[index])

    def attend(layer, g, wanted):
        cols = slice(g * group, (g + 1) * group)
        scores, weights, sums = {}, {}, {}
        for row in wanted:
            low = row * GRID_W
            q = qbuf[low : low + GRID_W, cols]
            if per_group == 2:
                zero = jnp.zeros_like(q)
                q = jnp.concatenate(
                    [
                        jnp.where(lane < HEAD_DIM, q, zero),
                        jnp.where(lane >= HEAD_DIM, q, zero),
                    ],
                    axis=0,
                )
            k = kvbuf[layer, g, low : low + KEYS, 0:group]
            scores[row] = lax.dot_general(
                q, k, (((1,), (1,)), ((), ())), preferred_element_type=F32
            )
        for row in wanted:
            exps = []
            sums[row] = []
            for i in range(per_group):
                head = g * per_group + i
                s = (
                    scores[row][i * GRID_W : (i + 1) * GRID_W]
                    + table[layer, head * GRID_W : (head + 1) * GRID_W, :]
                    + maskbuf[row]
                )
                e = jnp.exp(s - jnp.max(s, axis=-1, keepdims=True))
                sums[row].append(jnp.sum(e, axis=-1, keepdims=True))
                exps.append(e.astype(BF16))
            weights[row] = exps[0] if per_group == 1 else jnp.concatenate(exps, axis=0)
        for row in wanted:
            low = row * GRID_W
            v = kvbuf[layer, g, low : low + KEYS, group:]
            mixed = jnp.dot(weights[row], v, preferred_element_type=F32)
            parts = [
                mixed[i * GRID_W : (i + 1) * GRID_W] / sums[row][i] for i in range(per_group)
            ]
            result = (
                parts[0] if per_group == 1 else jnp.where(lane < HEAD_DIM, parts[0], parts[1])
            )
            att[layer, mine, g, low : low + GRID_W, :] = result.astype(BF16)

    chunk = CHUNK
    for layer in range(layers):
        source = stream_ref if layer == 0 else hbuf

        block = 32

        def norm_rows(i, carry):
            at = pl.ds(pl.multiple_of(i * block, block), block)
            x = source[at, :].astype(F32)
            inverse = lax.rsqrt(jnp.mean(x * x, axis=-1, keepdims=True) + EPS)
            nbuf[at, :] = (x * inverse * norm_gain_ref[layer : layer + 1, :]).astype(BF16)
            return carry

        lax.fori_loop(0, tokens // block, norm_rows, 0)

        k_gain = k_gain_ref[layer : layer + 1, :]
        q_gain = q_gain_ref[layer : layer + 1, :] * HEAD_DIM ** (-0.5)

        for g in range(groups):
            wkv_copy(layer, g, 0).wait()
            wkv_copy(layer, g, 1).wait()
            if layer == 0 and g == 0:
                wq_copy(0).start()
                wo_copy(0).start()
            own = slice(LOW, LOW + tokens)
            if paired:
                raw = jnp.dot(nbuf[...], wkvbuf[layer, g], preferred_element_type=F32)
                k_raw, v_raw = raw[:, 0:group], raw[:, group:]
            else:
                k_raw = jnp.dot(nbuf[...], wkvbuf[layer, 0], preferred_element_type=F32)
                v_raw = jnp.dot(nbuf[...], wkvbuf[layer, 1], preferred_element_type=F32)
            kvbuf[layer, g, own, 0:group] = head_norm(k_raw, k_gain)
            kvbuf[layer, g, own, group:] = v_raw.astype(BF16)
            if layer == 0 and g == 0:
                degree = has_prev.astype(jnp.int32) + has_next.astype(jnp.int32) + (tp_size - 1)
                pl.semaphore_wait(barrier, degree)
                start_both(mark_copies())
            start_both(halo(layer, g))

        if layer == 0:
            for later in range(1, layers):
                for g in range(groups):
                    wkv_copy(later, g, 0).start()
                    wkv_copy(later, g, 1).start()
                wq_copy(later).start()
                wo_copy(later).start()

        wq_copy(layer).wait()
        for start in range(0, head_width, span):
            cols = slice(start, start + span)
            raw = jnp.dot(nbuf[...], wqbuf[layer, :, cols], preferred_element_type=F32)
            qbuf[:, cols] = head_norm(raw, q_gain)
        if layer == 0:
            build_tables()
            wait_low(mark_copies())
            wait_high(mark_copies())
            build_masks()

        def attend_group(g):
            copies = halo(layer, g)
            wait_low(copies)
            wait_high(copies)
            count = rows // pieces_of(g)
            for piece in range(pieces_of(g)):
                attend(layer, g, range(piece * count, (piece + 1) * count))
                for step in range(1, tp_size):
                    att_copy(layer, g, step, piece).start()

        def add_part(step, part, first, last):
            owner = lax.rem(mine + tp_size - step, tp_size)
            size = len(part) * group
            begin = owner * head_width + part[0] * group
            at = pl.ds(pl.multiple_of(begin, HEAD_DIM), size)
            if step > 0:
                for g in part:
                    for piece in range(pieces_of(g)):
                        att_copy(layer, g, step, piece).wait_recv()
            pieces = [att[layer, owner, g] for g in part]
            heads_in = pieces[0] if len(pieces) == 1 else jnp.concatenate(pieces, axis=1)
            for start in range(0, width, chunk):
                cols = slice(start, start + chunk)
                total = jnp.dot(
                    heads_in,
                    wobuf[layer, at, cols],
                    preferred_element_type=F32,
                )
                total += source[:, cols].astype(F32) if first else acc[:, cols]
                if last:
                    hbuf[:, cols] = total.astype(BF16)
                    if layer == layers - 1 and start > 0:
                        out_copy(start // chunk - 1).start()
                else:
                    acc[:, cols] = total

        every = list(range(groups))
        half = groups // 2
        parts = [every[:half], every[half:]] if half else [every]
        pending = []
        for index, part in enumerate(parts):
            for g in part:
                attend_group(g)
                for job in pending:
                    add_part(*job)
                pending = []
            if index == 0:
                wo_copy(layer).wait()
            final = index == len(parts) - 1
            add_part(0, part, index == 0, final and tp_size == 1)
            pending = [
                (step, part, False, final and step == tp_size - 1)
                for step in range(1, tp_size)
            ]
        for job in pending:
            add_part(*job)

    out_copy(width // chunk - 1).start()
    wait_send_both(mark_copies())
    for layer in range(layers):
        for g in range(groups):
            wait_send_both(halo(layer, g))
            for step in range(1, tp_size):
                for piece in range(pieces_of(g)):
                    att_copy(layer, g, step, piece).wait_send()
    for index in range(width // CHUNK):
        out_copy(index).wait()


def on_device(
    sp_size,
    tp_size,
    stream,
    doc_ids,
    norm_gain,
    w_query,
    w_key,
    w_value,
    query_gain,
    key_gain,
    offset_bias,
    w_output,
):
    tokens, width = stream.shape
    layers, _, head_width = w_query.shape
    heads = head_width // HEAD_DIM
    rows = tokens // GRID_W
    all_width = w_output.shape[1]
    group = min(128, head_width)
    groups = head_width // group
    vmem = pl.BlockSpec(memory_space=pltpu.VMEM)
    hbm = pl.BlockSpec(memory_space=pl.ANY)
    sem = pltpu.SemaphoreType.DMA
    peers = max(1, tp_size - 1)
    result = pl.pallas_call(
        functools.partial(kernel, sp_size, tp_size),
        out_shape=jax.ShapeDtypeStruct((tokens, width), BF16),
        in_specs=[vmem, vmem, vmem, hbm, hbm, hbm, vmem, vmem, vmem, hbm],
        out_specs=hbm,
        scratch_shapes=[
            pltpu.VMEM((layers, width, head_width), BF16),
            pltpu.VMEM(
                (layers, groups, width, 256) if group == 128 else (layers, 2, width, group), BF16
            ),
            pltpu.VMEM((layers, all_width, width), BF16),
            pltpu.VMEM((tokens, width), BF16),
            pltpu.VMEM((tokens, width), BF16),
            pltpu.VMEM((tokens, head_width), BF16),
            pltpu.VMEM((layers, groups, LOW + tokens + HIGH, 2 * group), BF16),
            pltpu.VMEM((layers, tp_size, groups, tokens, group), BF16),
            pltpu.VMEM((tokens, width), F32),
            pltpu.VMEM((layers, heads * GRID_W, KEYS), F32),
            pltpu.VMEM((rows, GRID_W, KEYS), F32),
            pltpu.VMEM((2, 1, tokens), jnp.int32),
            pltpu.VMEM((WIN_ROWS, 128), F32),
            sem((layers,)),
            sem((layers, groups, 2)),
            sem((layers,)),
            sem((2,)),
            sem((2,)),
            sem((layers, groups, 2)),
            sem((layers, groups, 2)),
            sem((layers, peers, groups, 2)),
            sem((layers, peers, groups, 2)),
            sem((width // CHUNK,)),
        ],
        compiler_params=pltpu.CompilerParams(
            collective_id=0, has_side_effects=True, vmem_limit_bytes=60 * 1024 * 1024
        ),
    )(
        stream,
        doc_ids.reshape(1, tokens),
        norm_gain,
        w_query,
        w_key,
        w_value,
        query_gain,
        key_gain,
        offset_bias,
        w_output,
    )
    spec = pl.BlockSpec((tokens // 4, width), lambda i: (i, 0))
    return pl.pallas_call(
        pass_on,
        grid=(4,),
        out_shape=jax.ShapeDtypeStruct((tokens, width), BF16),
        in_specs=[spec],
        out_specs=spec,
    )(result)


def pass_on(from_ref, to_ref):
    to_ref[...] = from_ref[...]


def solution(mesh):
    return jax.shard_map(
        functools.partial(on_device, mesh.shape["sp"], mesh.shape["tp"]),
        mesh=mesh,
        in_specs=(
            P("sp", None),
            P("sp"),
            P(),
            P(None, None, "tp"),
            P(None, None, "tp"),
            P(None, None, "tp"),
            P(),
            P(),
            P(None, "tp", None, None),
            P(),
        ),
        out_specs=P("sp", None),
        check_vma=False,
    )
```
